32 devices in a mesh: rep: 2 (over y), fs: 4 (over z), tp: 4 (over x, core).
Axes of the slice: x: 2, y: 2, z: 4, core: 2. Of those that a mesh axis runs over, the one named last changes fastest.
Arguments:
- tokens: bfloat16 [2048, 2048], P(('rep', 'fs')), may hold values from -6 to 6
- gate_weight: bfloat16 [2048, 2816], P('fs', 'tp'), may hold values from -0.125 to 0.125
- up_weight: bfloat16 [2048, 2816], P('fs', 'tp'), may hold values from -0.125 to 0.125
- down_weight: bfloat16 [2816, 2048], P('tp', 'fs'), may hold values from -0.109375 to 0.109375
- out_grad: bfloat16 [2048, 2048], P(('rep', 'fs')), may hold values from -6 to 6
Outputs:
- input_grad: bfloat16 [2048, 2048], P(('rep', 'fs'))
- down_grad: float32 [2816, 2048], P('tp', 'fs')
- row_norms: float32 [2816], P('tp')
The draws below stay inside these ranges and needn't reach their ends.
All inputs are finite; a program needn't handle non-finite values.
Results may differ from the reference program's by a relative error of at most 0.024.
Values may be sent and summed in bfloat16 or wider, within the bound.
A program may use at most 64 MiB of HBM per device.

```python
import jax
import jax.numpy as jnp
from jax import lax

D = 2048
FF = 2816
TOKENS = 2048
N_TP = 4


def spiked(drawn, rng, source, target, parts, factor):
    def block_of(axis_at):
        return (jnp.arange(drawn.shape[axis_at]) // (drawn.shape[axis_at] // parts)).reshape((-1,) + (1,) * (drawn.ndim - 1 - axis_at))

    first = jax.random.permutation(rng, parts)[block_of(target)]
    second = (block_of(target) + parts // 2) % parts
    return jnp.where((block_of(source) == first) | (block_of(source) == second), factor * drawn, drawn)


def steps_of(own_key, dims, split, least, largest):
    def one(dim, blocks):
        steps = jax.random.uniform(jax.random.fold_in(jax.random.fold_in(own_key, 6), dim), (blocks,), jnp.float32, least / len(split), largest / len(split))
        return jnp.repeat(jnp.exp(steps), dims[dim] // blocks).reshape((-1,) + (1,) * (len(dims) - dim - 1))

    loudness = one(*split[0])
    for cut in split[1:]:
        loudness = loudness * one(*cut)
    return loudness


def noise(stream_key, extent, width, most, pieces=(), kind=jnp.bfloat16):
    entries = jax.random.normal(stream_key, extent, jnp.float32) * width
    if len(pieces) > 0:
        entries = steps_of(stream_key, extent, pieces, -0.22, 0.18) * entries
    return jnp.clip(entries, min=-most, max=most).astype(kind)


def noise_with(rng, dims, scale, bound, cuts, heavy, held_as=jnp.bfloat16):
    drawn = scale * jax.random.normal(rng, dims, jnp.float32)
    if cuts:
        drawn = drawn * steps_of(rng, dims, cuts, -0.22, 0.18)
    return jnp.clip(spiked(drawn, jax.random.fold_in(rng, 3), *heavy), -bound, bound).astype(held_as)


def setup_inputs(seed: int = 0) -> dict:
    key_of = jax.random.split(jax.random.key(seed), 6)
    tokens = noise(key_of[0], (TOKENS, D), 1.0, 6.0, ((0, 8),))
    gate_weight = noise(key_of[1], (D, FF), D ** -0.5, 0.125, ((0, 4), (1, 4)))
    up_weight = noise(key_of[2], (D, FF), D ** -0.5, 0.125, ((0, 4), (1, 4)))
    down_weight = noise(key_of[3], (FF, D), FF ** -0.5, 0.109375, ((0, 4), (1, 4)))
    out_grad = noise_with(key_of[4], (TOKENS, D), 1.0, 6.0, ((0, 8),), (0, 1, 8, 2.0))
    return {"tokens": tokens, "gate_weight": gate_weight, "up_weight": up_weight, "down_weight": down_weight, "out_grad": out_grad}


def reference(tokens, gate_weight, up_weight, down_weight, out_grad):
    gate_pre = jnp.dot(tokens, gate_weight, preferred_element_type=jnp.float32)
    up_pre = jnp.dot(tokens, up_weight, preferred_element_type=jnp.float32)
    sigma = jax.nn.sigmoid(gate_pre)
    activated = gate_pre * sigma
    hidden = (activated * up_pre).astype(jnp.bfloat16)
    hid_grad = lax.dot_general(out_grad, down_weight, (((1,), (1,)), ((), ())), preferred_element_type=jnp.float32)
    up_grad = (hid_grad * activated).astype(jnp.bfloat16)
    gate_grad = (hid_grad * up_pre * sigma * (1.0 + gate_pre * (1.0 - sigma))).astype(jnp.bfloat16)
    block = FF // N_TP

    def add_block(index, total):
        offset = (index * block).astype(jnp.int32)
        gate_part = lax.dynamic_slice_in_dim(gate_grad, offset, block, 1)
        up_part = lax.dynamic_slice_in_dim(up_grad, offset, block, 1)
        gate_rows = lax.dynamic_slice_in_dim(gate_weight, offset, block, 1)
        up_rows = lax.dynamic_slice_in_dim(up_weight, offset, block, 1)
        partial_value = lax.dot_general(gate_part, gate_rows, (((1,), (1,)), ((), ())), preferred_element_type=jnp.float32)
        partial_value = partial_value + lax.dot_general(up_part, up_rows, (((1,), (1,)), ((), ())), preferred_element_type=jnp.float32)
        return total + partial_value.astype(jnp.bfloat16).astype(jnp.float32)

    total = lax.fori_loop(0, N_TP, add_block, jnp.zeros(tokens.shape, jnp.float32))
    input_grad = total.astype(jnp.bfloat16)
    down_grad = lax.dot_general(hidden, out_grad, (((0,), (0,)), ((), ())), preferred_element_type=jnp.float32)
    row_norms = jnp.sum(down_grad * down_grad, axis=1)
    return input_grad, down_grad, row_norms
```

```python
import jax
import jax.numpy as jnp
from jax import lax
from jax.experimental import pallas as pl
from jax.experimental.pallas import tpu as pltpu
from jax.sharding import PartitionSpec as P

MESH = pl.DeviceIdType.MESH
BF16 = jnp.bfloat16
F32 = jnp.float32


def contract_last(left, right):
    return lax.dot_general(left, right, (((1,), (1,)), ((), ())), preferred_element_type=F32)


def contract_first(left, right):
    return lax.dot_general(left, right, (((0,), (0,)), ((), ())), preferred_element_type=F32)


def block_kernel(
    gate, up, down, tokens, grad, input_grad, down_grad, norms,
    gate_all, up_all, down_all, tokens_all, grad_all,
    gate_pre, up_pre, hid, gate_grad, up_grad, hid_all, hid_out,
    part, part_own, d_in, d_pass,
    f_out, f_in, g_own, g_out, g_in, h_out, h_in, whole_out, s_own, s_other, n_own, n_in,
    own_sem, w_send, w_recv, w_pass, y_send, y_recv, t_send, t_recv, hid_send, hid_recv,
    d_send, d_recv, e_send, e_recv, g_send, g_recv, s_send, s_recv, n_send, n_recv,
):
    n = 4
    f = lax.axis_index("fs")
    r = lax.axis_index("rep")
    t = lax.axis_index("tp")
    c, x = lax.rem(t, 2), t // 2
    h = lax.rem(f, 2)
    middle = (f == 1) | (f == 2)
    mate, far, pair = {"tp": x * 2 + 1 - c}, {"tp": (1 - x) * 2 + c}, {"rep": 1 - r}
    other = (f, f + 1 - 2 * h, lax.rem(f + 2, n), n - 1 - f)
    rows, depth = tokens.shape
    width = gate.shape[1]
    units, sub = gate_all.shape[0], hid_out.shape[1]
    half, quarter = depth // 2, rows // 4
    pieces = g_out.shape[0]
    size = half // pieces
    strip = width // 2
    shards = ((gate, gate_all), (up, up_all), (down, down_all))

    def cols(start, size):
        return pl.ds(pl.multiple_of(start, size), size)

    def tile(start, size):
        return pl.ds(pl.multiple_of(start, 16), size)

    def remote(src, dst, send, recv, peer):
        return pltpu.make_async_remote_copy(
            src_ref=src, dst_ref=dst, send_sem=send, recv_sem=recv,
            device_id=peer, device_id_type=MESH,
        )

    local = []
    places = [(tokens, tokens_all.at[pl.ds(0, rows)]), (grad, grad_all.at[pl.ds(0, rows)])]
    for own, whole in shards:
        for b in range(2):
            places.append((
                own.at[tile(h * units + (r if b == 0 else 1 - r) * sub, sub)],
                whole.at[pl.ds(b * sub, sub), cols(f * width, width)],
            ))
    for i, (own, place) in enumerate(places):
        copy = pltpu.make_async_copy(own, place, own_sem.at[i])
        copy.start()
        local.append(copy)

    barrier = pltpu.get_barrier_semaphore()
    peers = [{"rep": lax.rem(r + a, 2), "fs": other[k]}
             for a in range(2) for k in range(n) if a or k]
    for peer in peers + [mate, far]:
        pl.semaphore_signal(barrier, inc=1, device_id=peer, device_id_type=MESH)
    pl.semaphore_wait(barrier, 2 * n + 1)

    def slot(w, k):
        return shards[w][1].at[pl.ds(0, sub), cols(other[k] * width, width)]

    def weight(w, k):
        own, whole = shards[w]
        start = (h if k == 2 else 1 - h) * units + r * sub
        return remote(
            own.at[tile(start, sub)], whole.at[pl.ds(0, sub), cols(f * width, width)],
            w_send.at[w, k], w_recv.at[w, k], {"fs": other[k]},
        )

    def relay(w):
        return remote(slot(w, 1), slot(w, 1), w_pass.at[w], w_recv.at[w, 3], {"fs": other[2]})

    def across(w, k):
        place = cols(other[k] * width, width)
        return remote(
            shards[w][1].at[pl.ds(0, sub), place], shards[w][1].at[pl.ds(sub, sub), place],
            y_send.at[w, k], y_recv.at[w, k], pair,
        )

    def give(w, ks):
        for k in ks:
            if k == 3:
                @pl.when(middle)
                def _():
                    weight(w, k).start()
            else:
                weight(w, k).start()

    def arrive(w, k):
        weight(w, k).wait_recv()
        across(w, k).start()
        if k == 1:
            @pl.when(middle)
            def _():
                relay(w).start()

    flows = ((tokens, tokens_all, 1), (grad, grad_all, 1), (grad, grad_all, 2), (grad, grad_all, 3))

    def span(i, q):
        return flows[i][1].at[tile(flows[i][2] * rows + q * quarter, quarter)]

    q_near, q_far, q_mate, q_cross = t, (1 - x) * 2 + c, x * 2 + 1 - c, (1 - x) * 2 + 1 - c

    def fetch(i):
        own = grad_all.at[tile(rows + t * quarter, quarter)] if i == 3 else (
            flows[i][0].at[tile(t * quarter, quarter)])
        return remote(own, span(i, q_near), t_send.at[i, 0], t_recv.at[i, 0],
                      {"fs": other[1]} if i < 2 else pair)

    def spread(i, j):
        q = q_near if j < 3 else q_far
        return remote(span(i, q), span(i, q), t_send.at[i, j], t_recv.at[i, j],
                      far if j == 1 else mate)

    def hand(i):
        fetch(i).wait_recv()
        spread(i, 1).start()
        spread(i, 2).start()

    def pass_on(i):
        spread(i, 1).wait_recv()
        spread(i, 3).start()

    def complete(i):
        spread(i, 2).wait_recv()
        spread(i, 3).wait_recv()

    fetch(0).start()
    fetch(2).start()
    give(0, (1, 2, 3))
    fetch(1).start()
    give(1, (1, 2, 3))

    def pre(w, k):
        at = cols(other[k] * width, width)
        target = gate_pre if w == 0 else up_pre
        product = contract_last(tokens_all[:, at], shards[w][1][:, at])
        if k == 0:
            target[...] = product
        else:
            target[...] += product

    hand(0)
    hand(2)
    arrive(0, 1)
    pass_on(0)
    hand(1)
    fetch(3).start()
    arrive(1, 1)
    give(2, (1, 2, 3))
    pass_on(2)
    for copy in local:
        copy.wait()
    complete(0)
    for w in range(2):
        pre(w, 0)
    arrive(0, 2)
    pass_on(1)
    hand(3)
    arrive(1, 2)
    for w in range(2):
        across(w, 1).wait_recv()
        pre(w, 1)
    pass_on(3)
    arrive(0, 3)
    for w in range(2):
        across(w, 2).wait_recv()
        pre(w, 2)
    arrive(2, 1)
    arrive(1, 3)
    for w in range(2):
        across(w, 3).wait_recv()
        pre(w, 3)

    gated, raw = gate_pre[...], up_pre[...]
    sigma = jax.nn.sigmoid(gated)
    hidden = (gated * sigma * raw).astype(BF16)
    hid_out[...] = hidden[:, sub:]
    hid_swap = remote(hid_out, hid_all.at[pl.ds(2 * rows, 2 * rows)],
                      hid_send.at[0], hid_recv.at[0], pair)
    hid_swap.start()
    hid_all[pl.ds(0, 2 * rows)] = hidden[:, :sub]
    gate_pre[...] = gated * sigma
    up_pre[...] = raw * sigma * (1.0 + gated * (1.0 - sigma))

    def add_hid(k):
        at = cols(other[k] * width, width)
        product = contract_last(grad_all[pl.ds(0, 2 * rows), at], down_all[:, at])
        if k == 0:
            hid[...] = product
        else:
            hid[...] += product

    complete(1)
    add_hid(0)
    across(2, 1).wait_recv()
    add_hid(1)
    arrive(2, 2)

    def d_direct(k):
        return remote(part.at[k], d_in.at[k], d_send.at[k], d_recv.at[k], {"fs": other[k]})

    def d_first(k):
        return remote(part.at[k], d_pass.at[k], d_send.at[k], e_recv.at[k], {"fs": other[1]})

    def d_second(k):
        return remote(d_pass.at[k], d_in.at[k], e_send.at[k], d_recv.at[k], {"fs": other[5 - k]})

    complete(2)
    complete(3)
    hid_swap.wait_recv()
    for k in (2, 3, 1, 0):
        at = cols(other[k] * width, width)
        product = contract_first(hid_all[...], grad_all[:, at])
        if k == 0:
            part_own[...] = product
        else:
            part[k] = product.astype(BF16)
            if k == 1:
                d_direct(k).start()
            else:
                @pl.when(middle)
                def _():
                    d_direct(k).start()

                @pl.when(~middle)
                def _():
                    d_first(k).start()

    across(2, 2).wait_recv()
    add_hid(2)

    @pl.when(middle)
    def _():
        for k in (2, 3):
            d_first(k).wait_recv()
            d_second(k).start()

    arrive(2, 3)
    across(2, 3).wait_recv()
    add_hid(3)

    for b in (1, 0):
        at = pl.ds(b * rows, rows)
        up_grad[at] = (hid[at] * gate_pre[at]).astype(BF16)
        gate_grad[at] = (hid[at] * up_pre[at]).astype(BF16)

    def flow(b, at):
        block = pl.ds(b * rows, rows)
        return (
            jnp.dot(gate_grad[block], gate_all[:, at], preferred_element_type=F32)
            + jnp.dot(up_grad[block], up_all[:, at], preferred_element_type=F32)
        )

    def push(i, src, dst, peer):
        copy = remote(src, dst, g_send.at[i], g_recv.at[i], peer)
        copy.start()
        return copy

    neighbour = {"fs": other[1]}
    cross = {}
    for b in (1, 0):
        f_out[b] = flow(b, cols((1 - c) * half, half)).astype(BF16)
        cross[b] = push(b, f_out.at[b], f_in.at[b], mate)
    over = []
    for b in (1, 0):
        kept = flow(b, cols(c * half, half))
        cross[b].wait()
        kept = kept + f_in[b].astype(F32)
        for q in range(pieces):
            piece = kept[:, q * size:(q + 1) * size]
            if b == 1:
                g_out[q] = piece.astype(BF16)
                over.append(push(2 + q, g_out.at[q], g_in.at[q], neighbour))
            else:
                g_own[q] = piece
    sent = []
    for q in range(pieces):
        over[q].wait()
        h_out[q] = (g_own[q] + g_in[q].astype(F32)).astype(BF16)
        sent.append(push(2 + pieces + q, h_out.at[q], h_in.at[q], far))

    for k in range(1, n):
        d_direct(k).wait_recv()
    s_own[0] = (part_own[...] + d_in[2].astype(F32)).astype(BF16)
    s_own[1] = (d_in[1].astype(F32) + d_in[3].astype(F32)).astype(BF16)
    swap = remote(s_own, s_other, s_send.at[0], s_recv.at[0], pair)
    swap.start()
    sums = []
    for b in range(2):
        kept = s_own[b].astype(F32)
        down_grad[tile((h if b == 0 else 1 - h) * units + r * sub, sub)] = s_own[b]
        sums.append(lax.dot_general(
            jnp.ones((8, width), F32), kept * kept, (((1,), (1,)), ((), ())),
            precision=lax.Precision.HIGHEST, preferred_element_type=F32,
        ))
    n_own[...] = jnp.concatenate(
        [jnp.where(h == 0, sums[0], sums[1]), jnp.where(h == 0, sums[1], sums[0])], axis=1
    )
    small = []
    for i, peer in enumerate(peers):
        copy = remote(n_own, n_in.at[i], n_send.at[i], n_recv.at[i], peer)
        copy.start()
        small.append(copy)

    beside = []
    for q in range(pieces):
        sent[q].wait()
        at = cols(c * half + q * size, size)
        whole_out[:, at] = (h_out[q].astype(F32) + h_in[q].astype(F32)).astype(BF16)
        beside.append(push(2 + 2 * pieces + q, whole_out.at[:, at], whole_out.at[:, at], mate))

    for w in range(3):
        for k in (1, 2):
            weight(w, k).wait_send()

        @pl.when(middle)
        def _():
            weight(w, 3).wait_send()
            relay(w).wait_send()

        for k in range(1, n):
            across(w, k).wait_send()
    for i in range(4):
        fetch(i).wait_send()
        for j in range(1, 4):
            spread(i, j).wait_send()
    hid_swap.wait_send()
    for k in range(1, n):
        d_direct(k).wait_send()

    @pl.when(middle)
    def _():
        for k in (2, 3):
            d_second(k).wait_send()

    for copy in small:
        copy.wait()
    here = n_own[...]
    for i in range(n - 1):
        here = here + n_in[i]
    there = n_in[n - 1]
    for i in range(n, 2 * n - 1):
        there = there + n_in[i]
    first, second = jnp.where(r == 0, here, there), jnp.where(r == 0, there, here)
    norms[...] = jnp.concatenate(
        [first[:, :sub], second[:, :sub], first[:, sub:], second[:, sub:]], axis=1
    )
    swap.wait()
    for b in range(2):
        down_grad[tile((h if b == 0 else 1 - h) * units + (1 - r) * sub, sub)] = s_other[b]
    for copy in beside:
        copy.wait()
    input_grad[...] = whole_out[...]


def write_kernel(flow, shard, rows, input_grad, down_grad, norms):
    input_grad[...] = flow[...]
    down_grad[...] = shard[...].astype(F32)
    norms[...] = rows[0]


def split_units(tokens, gate_weight, up_weight, down_weight, out_grad):
    rows, depth = tokens.shape
    width, both = gate_weight.shape
    units, sub = both // 2, both // 4
    anywhere = pl.BlockSpec(memory_space=pl.ANY)
    vmem = pl.BlockSpec(memory_space=pltpu.VMEM)
    dma = pltpu.SemaphoreType.DMA
    n, half, pieces = 4, depth // 2, 4
    piece = (pieces, rows, half // pieces)
    peers = 2 * n - 1
    scratch = [((units, depth), BF16)] * 3 + [((2 * rows, depth), BF16), ((4 * rows, depth), BF16)]
    scratch += [((2 * rows, units), F32)] * 3 + [((2 * rows, units), BF16)] * 2
    scratch += [((4 * rows, sub), BF16), ((2 * rows, sub), BF16)]
    scratch += [((n, sub, width), BF16), ((sub, width), F32)] + [((n, sub, width), BF16)] * 2
    scratch += [((2, rows, half), BF16)] * 2 + [(piece, F32)] + [(piece, BF16)] * 4
    scratch += [((rows, depth), BF16)] + [((2, sub, width), BF16)] * 2
    scratch += [((8, units), F32), ((peers, 8, units), F32)]
    input_grad, down_grad, norms = pl.pallas_call(
        block_kernel,
        out_shape=[
            jax.ShapeDtypeStruct((rows, depth), BF16),
            jax.ShapeDtypeStruct((both, width), BF16),
            jax.ShapeDtypeStruct((8, both), F32),
        ],
        in_specs=[anywhere] * 5,
        out_specs=[vmem] * 3,
        scratch_shapes=[pltpu.VMEM(shape, kind) for shape, kind in scratch] + [
            dma((8,)), dma((3, n)), dma((3, n)), dma((3,)), dma((3, n)), dma((3, n)),
            dma((4, 4)), dma((4, 4)), dma((1,)), dma((1,)),
            dma((n,)), dma((n,)), dma((n,)), dma((n,)),
            dma((2 + 3 * pieces,)), dma((2 + 3 * pieces,)),
            dma((1,)), dma((1,)), dma((peers,)), dma((peers,)),
        ],
        compiler_params=pltpu.CompilerParams(collective_id=0, has_side_effects=True),
        name="block",
    )(gate_weight.T, up_weight.T, down_weight, tokens, out_grad)
    return tuple(pl.pallas_call(
        write_kernel,
        out_shape=[
            jax.ShapeDtypeStruct((rows, depth), BF16),
            jax.ShapeDtypeStruct((both, width), F32),
            jax.ShapeDtypeStruct((both,), F32),
        ],
        in_specs=[vmem] * 3,
        out_specs=[vmem] * 3,
        name="write",
    )(input_grad, down_grad, norms))


def whole_units(tokens, gate_weight, up_weight, down_weight, out_grad):
    down_full = lax.all_gather(down_weight, "fs", axis=1, tiled=True)
    gate_full = lax.all_gather(gate_weight, "fs", axis=0, tiled=True)
    up_full = lax.all_gather(up_weight, "fs", axis=0, tiled=True)
    gate_pre = jnp.dot(tokens, gate_full, preferred_element_type=F32)
    up_pre = jnp.dot(tokens, up_full, preferred_element_type=F32)
    sigma = jax.nn.sigmoid(gate_pre)
    activated = gate_pre * sigma
    hidden = (activated * up_pre).astype(BF16)
    hid_grad = contract_last(out_grad, down_full)
    up_grad = (hid_grad * activated).astype(BF16)
    gate_grad = (hid_grad * up_pre * sigma * (1.0 + gate_pre * (1.0 - sigma))).astype(BF16)
    partial_value = contract_last(gate_grad, gate_full) + contract_last(up_grad, up_full)
    input_grad = lax.psum(partial_value.astype(BF16), "tp")
    columns = lax.all_to_all(out_grad, "fs", split_axis=1, concat_axis=0, tiled=True)
    shard = contract_first(lax.all_gather(hidden, "fs", axis=0, tiled=True), columns)
    shard = lax.psum(shard.astype(BF16), "rep").astype(F32)
    norms = lax.psum(jnp.sum(shard * shard, axis=1), "fs")
    return (input_grad, shard, norms)


def solution(mesh):
    n, rep, tp = mesh.shape["fs"], mesh.shape["rep"], mesh.shape["tp"]

    def on_device(tokens, gate_weight, up_weight, down_weight, out_grad):
        width, both = gate_weight.shape
        if rep == 2 and tp == 4 and n == 4 and both % 64 == 0 and width % 256 == 0 and tokens.shape[0] % 64 == 0:
            return split_units(tokens, gate_weight, up_weight, down_weight, out_grad)
        return whole_units(tokens, gate_weight, up_weight, down_weight, out_grad)

    return jax.shard_map(
        on_device,
        mesh=mesh,
        in_specs=(
            P(("rep", "fs"), None),
            P("fs", "tp"),
            P("fs", "tp"),
            P("tp", "fs"),
            P(("rep", "fs"), None),
        ),
        out_specs=(P(("rep", "fs"), None), P("tp", "fs"), P("tp")),
        check_vma=False,
    )
```

```python
import jax
import jax.numpy as jnp
from jax import lax
from jax.experimental import pallas as pl
from jax.experimental.pallas import tpu as pltpu
from jax.sharding import PartitionSpec as P

MESH = pl.DeviceIdType.MESH
BF16 = jnp.bfloat16
F32 = jnp.float32


def contract_last(left, right):
    return lax.dot_general(left, right, (((1,), (1,)), ((), ())), preferred_element_type=F32)


def contract_first(left, right):
    return lax.dot_general(left, right, (((0,), (0,)), ((), ())), preferred_element_type=F32)


def block_kernel(
    gate, up, down, tokens, grad, input_grad, down_grad, norms,
    gate_all, up_all, down_all, tokens_all, grad_all,
    gate_pre, up_pre, hid, gate_grad, up_grad, hid_all, hid_out,
    part, part_own, d_in, d_pass,
    f_out, f_in, g_own, g_out, g_in, h_out, h_in, whole_out, s_own, s_other, n_own, n_in,
    own_sem, w_send, w_recv, w_pass, y_send, y_recv, t_send, t_recv, hid_send, hid_recv,
    d_send, d_recv, e_send, e_recv, g_send, g_recv, s_send, s_recv, n_send, n_recv,
):
    n = 4
    f = lax.axis_index("fs")
    r = lax.axis_index("rep")
    t = lax.axis_index("tp")
    c, x = lax.rem(t, 2), t // 2
    h = lax.rem(f, 2)
    middle = (f == 1) | (f == 2)
    mate, far, pair = {"tp": x * 2 + 1 - c}, {"tp": (1 - x) * 2 + c}, {"rep": 1 - r}
    other = (f, f + 1 - 2 * h, lax.rem(f + 2, n), n - 1 - f)
    rows, depth = tokens.shape
    width = gate.shape[1]
    units, sub = gate_all.shape[0], hid_out.shape[1]
    half, quarter = depth // 2, rows // 4
    pieces = g_out.shape[0]
    size = half // pieces
    shards = ((gate, gate_all), (up, up_all), (down, down_all))

    def cols(start, size):
        return pl.ds(pl.multiple_of(start, size), size)

    def tile(start, size):
        return pl.ds(pl.multiple_of(start, 16), size)

    def remote(src, dst, send, recv, peer):
        return pltpu.make_async_remote_copy(
            src_ref=src, dst_ref=dst, send_sem=send, recv_sem=recv,
            device_id=peer, device_id_type=MESH,
        )

    local = []
    places = [(tokens, tokens_all.at[pl.ds(0, rows)]), (grad, grad_all.at[pl.ds(0, rows)])]
    for own, whole in shards:
        for b in range(2):
            places.append((
                own.at[tile(h * units + (r if b == 0 else 1 - r) * sub, sub)],
                whole.at[pl.ds(b * sub, sub), cols(f * width, width)],
            ))
    for i, (own, place) in enumerate(places):
        copy = pltpu.make_async_copy(own, place, own_sem.at[i])
        copy.start()
        local.append(copy)

    barrier = pltpu.get_barrier_semaphore()
    peers = [{"rep": lax.rem(r + a, 2), "fs": other[k]}
             for a in range(2) for k in range(n) if a or k]
    for peer in peers + [mate, far]:
        pl.semaphore_signal(barrier, inc=1, device_id=peer, device_id_type=MESH)
    pl.semaphore_wait(barrier, 2 * n + 1)

    cuts = (1, 1, 2)

    def place(w, k, j):
        size = width // cuts[w]
        return cols(other[k] * width + j * size, size)

    def weight(w, k, j):
        own, whole = shards[w]
        start = (h if k == 2 else 1 - h) * units + r * sub
        size = width // cuts[w]
        return remote(
            own.at[tile(start, sub), pl.ds(j * size, size)],
            whole.at[pl.ds(0, sub), place(w, 0, j)],
            w_send.at[w, k, j], w_recv.at[w, k, j], {"fs": other[k]},
        )

    def relay(w, j):
        slot = shards[w][1].at[pl.ds(0, sub), place(w, 1, j)]
        return remote(slot, slot, w_pass.at[w, j], w_recv.at[w, 3, j], {"fs": other[2]})

    def across(w, k, j):
        whole = shards[w][1]
        return remote(
            whole.at[pl.ds(0, sub), place(w, k, j)], whole.at[pl.ds(sub, sub), place(w, k, j)],
            y_send.at[w, k, j], y_recv.at[w, k, j], pair,
        )

    flows = ((tokens, tokens_all, 1), (grad, grad_all, 1), (grad, grad_all, 2), (grad, grad_all, 3))

    def span(i, q):
        return flows[i][1].at[tile(flows[i][2] * rows + q * quarter, quarter)]

    q_near, q_far = t, (1 - x) * 2 + c

    def fetch(i):
        own = grad_all.at[tile(rows + t * quarter, quarter)] if i == 3 else (
            flows[i][0].at[tile(t * quarter, quarter)])
        return remote(own, span(i, q_near), t_send.at[i, 0], t_recv.at[i, 0],
                      {"fs": other[1]} if i < 2 else pair)

    def spread(i, j):
        q = q_near if j < 3 else q_far
        return remote(span(i, q), span(i, q), t_send.at[i, j], t_recv.at[i, j],
                      far if j == 1 else mate)

    def hand(i):
        fetch(i).wait_recv()
        spread(i, 1).start()
        spread(i, 2).start()

    def pass_on(i):
        spread(i, 1).wait_recv()
        spread(i, 3).start()

    def complete(i):
        spread(i, 2).wait_recv()
        spread(i, 3).wait_recv()

    def body(mid):
        def give(w, k):
            for j in range(cuts[w]):
                weight(w, k, j).start()

        def arrive(w, k):
            for j in range(cuts[w]):
                weight(w, k, j).wait_recv()
                if k == 1 and mid:
                    relay(w, j).start()
                across(w, k, j).start()

        def arrived(w, k):
            for j in range(cuts[w]):
                across(w, k, j).wait_recv()

        def pre(k):
            at = place(0, k, 0)
            for w, target in ((0, gate_pre), (1, up_pre)):
                if k:
                    arrived(w, k)
                product = contract_last(tokens_all[:, at], shards[w][1][:, at])
                if k == 0:
                    target[...] = product
                else:
                    target[...] += product

        def start_pre():
            for copy in local:
                copy.wait()
            complete(0)
            pre(0)

        hid_swap = remote(hid_out, hid_all.at[pl.ds(2 * rows, 2 * rows)],
                          hid_send.at[0], hid_recv.at[0], pair)

        def activate():
            gated, raw = gate_pre[...], up_pre[...]
            sigma = jax.nn.sigmoid(gated)
            hidden = (gated * sigma * raw).astype(BF16)
            hid_out[...] = hidden[:, sub:]
            hid_swap.start()
            hid_all[pl.ds(0, 2 * rows)] = hidden[:, :sub]
            gate_pre[...] = gated * sigma
            up_pre[...] = raw * sigma * (1.0 + gated * (1.0 - sigma))

        def add_hid(k):
            if k:
                arrived(2, k)
            else:
                complete(1)
            at = cols(other[k] * width, width)
            product = contract_last(grad_all[pl.ds(0, 2 * rows), at], down_all[:, at])
            if k == 0:
                hid[...] = product
            else:
                hid[...] += product

        def d_direct(k):
            return remote(part.at[k], d_in.at[k], d_send.at[k], d_recv.at[k], {"fs": other[k]})

        def d_first(k):
            return remote(part.at[k], d_pass.at[k], d_send.at[k], e_recv.at[k], {"fs": other[1]})

        def d_second(k):
            return remote(d_pass.at[k], d_in.at[k], e_send.at[k], d_recv.at[k], {"fs": other[5 - k]})

        def products():
            complete(2)
            complete(3)
            hid_swap.wait_recv()
            for k in (2, 3, 1, 0):
                at = cols(other[k] * width, width)
                product = contract_first(hid_all[...], grad_all[:, at])
                if k == 0:
                    part_own[...] = product
                    continue
                part[k] = product.astype(BF16)
                (d_direct if mid or k == 1 else d_first)(k).start()

        def hand_products():
            for k in (2, 3):
                d_first(k).wait_recv()
                d_second(k).start()

        def flow(b, at):
            span = pl.ds(b * rows, rows)
            return (
                jnp.dot(gate_grad[span], gate_all[:, at], preferred_element_type=F32)
                + jnp.dot(up_grad[span], up_all[:, at], preferred_element_type=F32)
            )

        def push(i, src, dst, peer):
            copy = remote(src, dst, g_send.at[i], g_recv.at[i], peer)
            copy.start()
            return copy

        def rows_done():
            for k in range(1, n):
                d_direct(k).wait_recv()
            s_own[0] = (part_own[...] + d_in[2].astype(F32)).astype(BF16)
            s_own[1] = (d_in[1].astype(F32) + d_in[3].astype(F32)).astype(BF16)
            sums = []
            for b in range(2):
                kept = s_own[b].astype(F32)
                down_grad[tile((h if b == 0 else 1 - h) * units + r * sub, sub)] = s_own[b]
                sums.append(lax.dot_general(
                    jnp.ones((8, width), F32), kept * kept, (((1,), (1,)), ((), ())),
                    precision=lax.Precision.HIGHEST, preferred_element_type=F32,
                ))
            n_own[...] = jnp.concatenate(
                [jnp.where(h == 0, sums[0], sums[1]), jnp.where(h == 0, sums[1], sums[0])], axis=1
            )
            small = []
            for i, peer in enumerate(peers):
                copy = remote(n_own, n_in.at[i], n_send.at[i], n_recv.at[i], peer)
                copy.start()
                small.append(copy)
            swap = remote(s_own, s_other, s_send.at[0], s_recv.at[0], pair)
            swap.start()
            return swap, small

        if mid:
            fetch(2).start()
            fetch(0).start()
            for k in (1, 3, 2):
                give(0, k)
            fetch(1).start()
            for k in (1, 3, 2):
                give(1, k)
            arrive(0, 1)
            arrive(0, 3)
            hand(0)
            arrive(1, 1)
            for k in (1, 3, 2):
                give(2, k)
            hand(2)
            arrive(1, 3)
            pass_on(0)
            start_pre()
            arrive(0, 2)
            pre(1)
            hand(1)
            fetch(3).start()
            pass_on(2)
            pre(3)
            arrive(1, 2)
            pass_on(1)
            hand(3)
            arrive(2, 1)
            pre(2)
            pass_on(3)
            activate()
            add_hid(0)
            add_hid(1)
            arrive(2, 3)
            arrive(2, 2)
            products()
            add_hid(3)
            add_hid(2)
        else:
            fetch(2).start()
            give(0, 1)
            fetch(0).start()
            give(1, 1)
            give(0, 2)
            fetch(1).start()
            give(1, 2)
            give(2, 1)
            give(2, 2)
            hand(2)
            arrive(0, 2)
            hand(0)
            arrive(0, 1)
            pass_on(0)
            arrive(1, 2)
            pass_on(2)
            hand(1)
            fetch(3).start()
            arrive(0, 3)
            pass_on(1)
            start_pre()
            hand(3)
            arrive(1, 1)
            arrive(1, 3)
            pre(2)
            pre(1)
            pre(3)
            activate()
            pass_on(3)
            arrive(2, 2)
            add_hid(0)
            arrive(2, 1)
            arrive(2, 3)
            products()
            add_hid(2)
            add_hid(1)
            add_hid(3)

        neighbour = {"fs": other[1]}
        cross = {}
        for b in (1, 0):
            at = pl.ds(b * rows, rows)
            up_grad[at] = (hid[at] * gate_pre[at]).astype(BF16)
            gate_grad[at] = (hid[at] * up_pre[at]).astype(BF16)
            f_out[b] = flow(b, cols((1 - c) * half, half)).astype(BF16)
            cross[b] = push(b, f_out.at[b], f_in.at[b], mate)
        over = []
        for b in (1, 0):
            kept = flow(b, cols(c * half, half))
            cross[b].wait()
            kept = kept + f_in[b].astype(F32)
            for q in range(pieces):
                piece = kept[:, q * size:(q + 1) * size]
                if b == 1:
                    g_out[q] = piece.astype(BF16)
                    over.append(push(2 + q, g_out.at[q], g_in.at[q], neighbour))
                else:
                    g_own[q] = piece
        if mid:
            hand_products()
        sent = []
        for q in range(pieces):
            over[q].wait()
            h_out[q] = (g_own[q] + g_in[q].astype(F32)).astype(BF16)
            sent.append(push(2 + pieces + q, h_out.at[q], h_in.at[q], far))
        swap, small = rows_done()
        beside = []
        for q in range(pieces):
            sent[q].wait()
            at = cols(c * half + q * size, size)
            whole_out[:, at] = (h_out[q].astype(F32) + h_in[q].astype(F32)).astype(BF16)
            beside.append(push(2 + 2 * pieces + q, whole_out.at[:, at], whole_out.at[:, at], mate))

        for w in range(3):
            for j in range(cuts[w]):
                for k in (1, 2, 3) if mid else (1, 2):
                    weight(w, k, j).wait_send()
                if mid:
                    relay(w, j).wait_send()
                for k in range(1, n):
                    across(w, k, j).wait_send()
        for i in range(4):
            fetch(i).wait_send()
            for j in range(1, 4):
                spread(i, j).wait_send()
        hid_swap.wait_send()
        for k in range(1, n):
            d_direct(k).wait_send()
        if mid:
            for k in (2, 3):
                d_second(k).wait_send()

        for copy in small:
            copy.wait()
        here = n_own[...]
        for i in range(n - 1):
            here = here + n_in[i]
        there = n_in[n - 1]
        for i in range(n, 2 * n - 1):
            there = there + n_in[i]
        first, second = jnp.where(r == 0, here, there), jnp.where(r == 0, there, here)
        norms[...] = jnp.concatenate(
            [first[:, :sub], second[:, :sub], first[:, sub:], second[:, sub:]], axis=1
        )
        swap.wait()
        for b in range(2):
            down_grad[tile((h if b == 0 else 1 - h) * units + (1 - r) * sub, sub)] = s_other[b]
        for copy in beside:
            copy.wait()
        input_grad[...] = whole_out[...]

    @pl.when(middle)
    def _():
        body(True)

    @pl.when(~middle)
    def _():
        body(False)


def write_kernel(flow, shard, rows, input_grad, down_grad, norms):
    input_grad[...] = flow[...]
    down_grad[...] = shard[...].astype(F32)
    norms[...] = rows[0]


def split_units(tokens, gate_weight, up_weight, down_weight, out_grad):
    rows, depth = tokens.shape
    width, both = gate_weight.shape
    units, sub = both // 2, both // 4
    anywhere = pl.BlockSpec(memory_space=pl.ANY)
    vmem = pl.BlockSpec(memory_space=pltpu.VMEM)
    dma = pltpu.SemaphoreType.DMA
    n, half, pieces = 4, depth // 2, 4
    piece = (pieces, rows, half // pieces)
    peers = 2 * n - 1
    scratch = [((units, depth), BF16)] * 3 + [((2 * rows, depth), BF16), ((4 * rows, depth), BF16)]
    scratch += [((2 * rows, units), F32)] * 3 + [((2 * rows, units), BF16)] * 2
    scratch += [((4 * rows, sub), BF16), ((2 * rows, sub), BF16)]
    scratch += [((n, sub, width), BF16), ((sub, width), F32)] + [((n, sub, width), BF16)] * 2
    scratch += [((2, rows, half), BF16)] * 2 + [(piece, F32)] + [(piece, BF16)] * 4
    scratch += [((rows, depth), BF16)] + [((2, sub, width), BF16)] * 2
    scratch += [((8, units), F32), ((peers, 8, units), F32)]
    input_grad, down_grad, norms = pl.pallas_call(
        block_kernel,
        out_shape=[
            jax.ShapeDtypeStruct((rows, depth), BF16),
            jax.ShapeDtypeStruct((both, width), BF16),
            jax.ShapeDtypeStruct((8, both), F32),
        ],
        in_specs=[anywhere] * 5,
        out_specs=[vmem] * 3,
        scratch_shapes=[pltpu.VMEM(shape, kind) for shape, kind in scratch] + [
            dma((8,)), dma((3, n, 2)), dma((3, n, 2)), dma((3, 2)), dma((3, n, 2)), dma((3, n, 2)),
            dma((4, 4)), dma((4, 4)), dma((1,)), dma((1,)),
            dma((n,)), dma((n,)), dma((n,)), dma((n,)),
            dma((2 + 3 * pieces,)), dma((2 + 3 * pieces,)),
            dma((1,)), dma((1,)), dma((peers,)), dma((peers,)),
        ],
        compiler_params=pltpu.CompilerParams(collective_id=0, has_side_effects=True),
        name="block",
    )(gate_weight.T, up_weight.T, down_weight, tokens, out_grad)
    return tuple(pl.pallas_call(
        write_kernel,
        out_shape=[
            jax.ShapeDtypeStruct((rows, depth), BF16),
            jax.ShapeDtypeStruct((both, width), F32),
            jax.ShapeDtypeStruct((both,), F32),
        ],
        in_specs=[vmem] * 3,
        out_specs=[vmem] * 3,
        name="write",
    )(input_grad, down_grad, norms))


def whole_units(tokens, gate_weight, up_weight, down_weight, out_grad):
    down_full = lax.all_gather(down_weight, "fs", axis=1, tiled=True)
    gate_full = lax.all_gather(gate_weight, "fs", axis=0, tiled=True)
    up_full = lax.all_gather(up_weight, "fs", axis=0, tiled=True)
    gate_pre = jnp.dot(tokens, gate_full, preferred_element_type=F32)
    up_pre = jnp.dot(tokens, up_full, preferred_element_type=F32)
    sigma = jax.nn.sigmoid(gate_pre)
    activated = gate_pre * sigma
    hidden = (activated * up_pre).astype(BF16)
    hid_grad = contract_last(out_grad, down_full)
    up_grad = (hid_grad * activated).astype(BF16)
    gate_grad = (hid_grad * up_pre * sigma * (1.0 + gate_pre * (1.0 - sigma))).astype(BF16)
    partial_value = contract_last(gate_grad, gate_full) + contract_last(up_grad, up_full)
    input_grad = lax.psum(partial_value.astype(BF16), "tp")
    columns = lax.all_to_all(out_grad, "fs", split_axis=1, concat_axis=0, tiled=True)
    shard = contract_first(lax.all_gather(hidden, "fs", axis=0, tiled=True), columns)
    shard = lax.psum(shard.astype(BF16), "rep").astype(F32)
    norms = lax.psum(jnp.sum(shard * shard, axis=1), "fs")
    return (input_grad, shard, norms)


def solution(mesh):
    n, rep, tp = mesh.shape["fs"], mesh.shape["rep"], mesh.shape["tp"]

    def on_device(tokens, gate_weight, up_weight, down_weight, out_grad):
        width, both = gate_weight.shape
        if rep == 2 and tp == 4 and n == 4 and both % 64 == 0 and width % 256 == 0 and tokens.shape[0] % 64 == 0:
            return split_units(tokens, gate_weight, up_weight, down_weight, out_grad)
        return whole_units(tokens, gate_weight, up_weight, down_weight, out_grad)

    return jax.shard_map(
        on_device,
        mesh=mesh,
        in_specs=(
            P(("rep", "fs"), None),
            P("fs", "tp"),
            P("fs", "tp"),
            P("tp", "fs"),
            P(("rep", "fs"), None),
        ),
        out_specs=(P(("rep", "fs"), None), P("tp", "fs"), P("tp")),
        check_vma=False,
    )
```

```python
import jax
import jax.numpy as jnp
from jax import lax
from jax.experimental import pallas as pl
from jax.experimental.pallas import tpu as pltpu
from jax.sharding import PartitionSpec as P

MESH = pl.DeviceIdType.MESH
BF16 = jnp.bfloat16
F32 = jnp.float32


def contract_last(left, right):
    return lax.dot_general(left, right, (((1,), (1,)), ((), ())), preferred_element_type=F32)


def contract_first(left, right):
    return lax.dot_general(left, right, (((0,), (0,)), ((), ())), preferred_element_type=F32)


def block_kernel(
    gate, up, down, tokens, grad, input_grad, down_grad, norms,
    gate_m, up_m, down_m, gate_e, up_e, down_e, tokens_all, grad_all,
    gate_pre, up_pre, hid, gate_grad, up_grad, hid_all_m, hid_out_m, hid_all_e, hid_out_e,
    part_m, part_e, part_own, d_in_m, d_in_e, d_pass,
    f_out, f_in, g_own, g_out, g_in, h_out, h_in, whole_out, s_own_m, s_own_e, s_other_m, s_other_e,
    n_own, n_in,
    own_sem, w_send, w_recv, w_pass, b_send, b_recv, y_send, y_recv, t_send, t_recv, hid_send, hid_recv,
    d_send, d_recv, e_send, e_recv, g_send, g_recv, s_send, s_recv, n_send, n_recv,
):
    n = 4
    f = lax.axis_index("fs")
    r = lax.axis_index("rep")
    t = lax.axis_index("tp")
    c, x = lax.rem(t, 2), t // 2
    middle = (f == 1) | (f == 2)
    mate, far, pair = {"tp": x * 2 + 1 - c}, {"tp": (1 - x) * 2 + c}, {"rep": 1 - r}
    other = (f, f + 1 - 2 * lax.rem(f, 2), lax.rem(f + 2, n), n - 1 - f)
    rows, depth = tokens.shape
    width = gate.shape[1]
    half, quarter = depth // 2, rows // 4
    pieces = g_out.shape[0]
    size = half // pieces
    owns = (gate, up, down)
    sub_m, sub_e = hid_out_m.shape[1], hid_out_e.shape[1]
    subs = {True: sub_m, False: sub_e}
    bases = {True: 2 * sub_e, False: 0}
    wholes = {True: (gate_m, up_m, down_m), False: (gate_e, up_e, down_e)}

    def cols(start, size):
        return pl.ds(pl.multiple_of(start, size), size)

    def tile(start, size):
        return pl.ds(pl.multiple_of(start, 16), size)

    def remote(src, dst, send, recv, peer):
        return pltpu.make_async_remote_copy(
            src_ref=src, dst_ref=dst, send_sem=send, recv_sem=recv,
            device_id=peer, device_id_type=MESH,
        )

    held = [
        pltpu.make_async_copy(own, whole.at[pl.ds(0, rows)], own_sem.at[i])
        for i, (own, whole) in enumerate(((tokens, tokens_all), (grad, grad_all)))
    ]

    def own_rows(mid):
        sub = subs[mid]
        return [
            pltpu.make_async_copy(
                own.at[tile(bases[mid] + (r if b == 0 else 1 - r) * sub, sub)],
                whole.at[pl.ds(b * sub, sub), cols(f * width, width)],
                own_sem.at[2 + 2 * w + b],
            )
            for w, (own, whole) in enumerate(zip(owns, wholes[mid])) for b in range(2)
        ]

    for copy in held:
        copy.start()

    barrier = pltpu.get_barrier_semaphore()
    peers = [{"rep": lax.rem(r + a, 2), "fs": other[k]}
             for a in range(2) for k in range(n) if a or k]
    for peer in peers + [mate, far]:
        pl.semaphore_signal(barrier, inc=1, device_id=peer, device_id_type=MESH)
    pl.semaphore_wait(barrier, 2 * n + 1)

    cuts = (1, 1, 2)

    def place(w, k, j):
        size = width // cuts[w]
        return cols(other[k] * width + j * size, size)

    flows = ((tokens, tokens_all, 1), (grad, grad_all, 1), (grad, grad_all, 2), (grad, grad_all, 3))

    def span(i, q):
        return flows[i][1].at[tile(flows[i][2] * rows + q * quarter, quarter)]

    q_near, q_far = t, (1 - x) * 2 + c

    def fetch(i):
        own = grad_all.at[tile(rows + t * quarter, quarter)] if i == 3 else (
            flows[i][0].at[tile(t * quarter, quarter)])
        return remote(own, span(i, q_near), t_send.at[i, 0], t_recv.at[i, 0],
                      {"fs": other[1]} if i < 2 else pair)

    def spread(i, j):
        q = q_near if j < 3 else q_far
        return remote(span(i, q), span(i, q), t_send.at[i, j], t_recv.at[i, j],
                      far if j == 1 else mate)

    def hand(i):
        fetch(i).wait_recv()
        spread(i, 1).start()
        spread(i, 2).start()

    def pass_on(i):
        spread(i, 1).wait_recv()
        spread(i, 3).start()

    def complete(i):
        spread(i, 2).wait_recv()
        spread(i, 3).wait_recv()

    def body(mid):
        sub = subs[mid]
        units = 2 * sub
        whole = wholes[mid]
        hid_all, hid_out, part = (hid_all_m, hid_out_m, part_m) if mid else (hid_all_e, hid_out_e, part_e)
        role = (mid, not mid, not mid, mid)
        local = held + own_rows(mid)
        for copy in local[2:]:
            copy.start()

        def weight(w, k, j, out=True):
            to = role[k] if out else mid
            rows_to, size = subs[to], width // cuts[w]
            return remote(
                owns[w].at[tile(bases[to] + r * rows_to, rows_to), pl.ds(j * size, size)],
                wholes[to][w].at[pl.ds(0, rows_to), place(w, 0 if out else k, j)],
                w_send.at[w, k, j], w_recv.at[w, k, j], {"fs": other[k]},
            )

        def second(w, j):
            size = width // cuts[w]
            return remote(
                owns[w].at[tile(bases[True] + (1 - r) * sub_m, sub_m), pl.ds(j * size, size)],
                wholes[True][w].at[pl.ds(sub_m, sub_m), place(w, 1 if mid else 0, j)],
                b_send.at[w, j], b_recv.at[w, j], {"fs": other[1]},
            )

        def relay(w, j):
            slot = whole[w].at[pl.ds(0, sub), place(w, 1, j)]
            return remote(slot, slot, w_pass.at[w, j], w_recv.at[w, 2, j], {"fs": other[3]})

        def across(w, k, j):
            return remote(
                whole[w].at[pl.ds(0, sub), place(w, k, j)], whole[w].at[pl.ds(sub, sub), place(w, k, j)],
                y_send.at[w, k, j], y_recv.at[w, k, j], pair,
            )

        def give(w, k):
            for j in range(cuts[w]):
                weight(w, k, j).start()

        def give_second(w):
            for j in range(cuts[w]):
                second(w, j).start()

        def arrive(w, k):
            for j in range(cuts[w]):
                weight(w, k, j, False).wait_recv()
                (relay(w, j) if mid and k == 1 else across(w, k, j)).start()

        def arrived(w, k):
            for j in range(cuts[w]):
                if mid and k == 1:
                    second(w, j).wait_recv()
                else:
                    across(w, k, j).wait_recv()

        def pre(k):
            at = place(0, k, 0)
            for w, target in ((0, gate_pre), (1, up_pre)):
                if k:
                    arrived(w, k)
                product = contract_last(tokens_all[:, at], whole[w][pl.ds(0, units), at])
                if k == 0:
                    target[:, :units] = product
                else:
                    target[:, :units] += product

        def start_pre():
            for copy in local:
                copy.wait()
            complete(0)
            pre(0)

        hid_swap = remote(hid_out, hid_all.at[pl.ds(2 * rows, 2 * rows)],
                          hid_send.at[0], hid_recv.at[0], pair)

        def activate():
            gated, raw = gate_pre[:, :units], up_pre[:, :units]
            sigma = jax.nn.sigmoid(gated)
            hidden = (gated * sigma * raw).astype(BF16)
            hid_out[...] = hidden[:, sub:]
            hid_all[pl.ds(0, 2 * rows)] = hidden[:, :sub]
            gate_pre[:, :units] = gated * sigma
            up_pre[:, :units] = raw * sigma * (1.0 + gated * (1.0 - sigma))

        def add_hid(k):
            if k:
                arrived(2, k)
            else:
                complete(1)
            at = cols(other[k] * width, width)
            product = contract_last(grad_all[pl.ds(0, 2 * rows), at], down_rows(at))
            if k == 0:
                hid[:, :units] = product
            else:
                hid[:, :units] += product

        def down_rows(at):
            return whole[2][pl.ds(0, units), at]

        def d_in(k, of):
            return (d_in_m if of else d_in_e).at[k]

        def d_direct(k):
            return remote(part.at[k], d_in(k, mid), d_send.at[k], d_recv.at[k], {"fs": other[k]})

        def d_done(k):
            return remote(d_in(k, role[k]), d_in(k, role[k]), d_send.at[k], d_recv.at[k], {"fs": other[k]})

        def d_first(k):
            return remote(part_e.at[k], d_pass.at[k], d_send.at[k], e_recv.at[k], {"fs": other[1]})

        def d_second(k):
            return remote(d_pass.at[k], d_in(k, False), e_send.at[k], d_recv.at[k], {"fs": other[5 - k]})

        def products():
            complete(2)
            complete(3)
            hid_swap.wait_recv()
            for k in (2, 3, 1, 0):
                at = cols(other[k] * width, width)
                product = contract_first(hid_all[...], grad_all[:, at])
                if k == 0:
                    part_own[pl.ds(0, sub)] = product
                    continue
                part[k] = product.astype(BF16)
                (d_direct if mid or k == 1 else d_first)(k).start()

        def hand_products():
            for k in (2, 3):
                d_first(k).wait_recv()
                d_second(k).start()

        def flow(b, at):
            span = pl.ds(b * rows, rows)
            return (
                jnp.dot(gate_grad[span, :units], whole[0][pl.ds(0, units), at],
                        preferred_element_type=F32)
                + jnp.dot(up_grad[span, :units], whole[1][pl.ds(0, units), at],
                          preferred_element_type=F32)
            )

        def push(i, src, dst, peer):
            copy = remote(src, dst, g_send.at[i], g_recv.at[i], peer)
            copy.start()
            return copy

        def rows_done():
            for k in range(1, n):
                d_done(k).wait_recv()
            sums = {}
            mine, others = (s_own_m, s_own_e) if mid else (s_own_e, s_own_m)
            mine[...] = (part_own[pl.ds(0, sub)] + d_in(3, mid)[...].astype(F32)).astype(BF16)
            others[...] = (
                d_in(1, not mid)[...].astype(F32) + d_in(2, not mid)[...].astype(F32)
            ).astype(BF16)
            for of, own in ((True, s_own_m), (False, s_own_e)):
                kept = own[...].astype(F32)
                down_grad[tile(bases[of] + r * subs[of], subs[of])] = own[...]
                sums[of] = lax.dot_general(
                    jnp.ones((8, width), F32), kept * kept, (((1,), (1,)), ((), ())),
                    precision=lax.Precision.HIGHEST, preferred_element_type=F32,
                )
            n_own[...] = jnp.concatenate([sums[False], sums[True]], axis=1)
            small = []
            for i, peer in enumerate(peers):
                copy = remote(n_own, n_in.at[i], n_send.at[i], n_recv.at[i], peer)
                copy.start()
                small.append(copy)
            swaps = []
            for i, (own, theirs) in enumerate(((s_own_m, s_other_m), (s_own_e, s_other_e))):
                copy = remote(own, theirs, s_send.at[i], s_recv.at[i], pair)
                copy.start()
                swaps.append(copy)
            return swaps, small

        if mid:
            fetch(2).start()
            fetch(0).start()
            give(0, 3)
            give(1, 3)
            give(0, 1)
            fetch(1).start()
            give(1, 1)
            arrive(0, 1)
            give(0, 2)
            give(1, 2)
            arrive(0, 3)
            hand(0)
            arrive(1, 3)
            hand(2)
            arrive(1, 1)
            for k in (1, 3, 2):
                give(2, k)
            pass_on(0)
            arrive(0, 2)
            start_pre()
            hand(1)
            fetch(3).start()
            pass_on(2)
            pre(3)
            arrive(1, 2)
            pass_on(1)
            hand(3)
            arrive(2, 3)
            pre(2)
            pre(1)
            activate()
            hid_swap.start()
            pass_on(3)
            arrive(2, 1)
            add_hid(0)
            add_hid(3)
            arrive(2, 2)
            products()
            add_hid(1)
            add_hid(2)
        else:
            fetch(2).start()
            give(0, 1)
            fetch(0).start()
            give(1, 1)
            give(0, 3)
            fetch(1).start()
            give(1, 3)
            give_second(0)
            give(2, 1)
            give_second(1)
            give(2, 3)
            give_second(2)
            hand(2)
            hand(0)
            arrive(0, 1)
            pass_on(2)
            pass_on(0)
            arrive(0, 3)
            arrive(0, 2)
            hand(1)
            fetch(3).start()
            start_pre()
            arrive(1, 2)
            arrive(1, 3)
            pass_on(1)
            arrive(1, 1)
            hand(3)
            pre(2)
            pre(1)
            arrive(2, 1)
            pre(3)
            activate()
            hid_swap.start()
            pass_on(3)
            arrive(2, 2)
            add_hid(0)
            products()
            add_hid(1)
            add_hid(2)
            arrive(2, 3)
            add_hid(3)

        neighbour = {"fs": other[1]}
        cross = {}
        for b in (1, 0):
            at = pl.ds(b * rows, rows)
            up_grad[at, :units] = (hid[at, :units] * gate_pre[at, :units]).astype(BF16)
            gate_grad[at, :units] = (hid[at, :units] * up_pre[at, :units]).astype(BF16)
            f_out[b] = flow(b, cols((1 - c) * half, half)).astype(BF16)
            cross[b] = push(b, f_out.at[b], f_in.at[b], mate)
        if mid:
            hand_products()
        over = []
        for b in (1, 0):
            kept = flow(b, cols(c * half, half))
            cross[b].wait()
            kept = kept + f_in[b].astype(F32)
            for q in range(pieces):
                piece = kept[:, q * size:(q + 1) * size]
                if b == 1:
                    g_out[q] = piece.astype(BF16)
                    over.append(push(2 + q, g_out.at[q], g_in.at[q], neighbour))
                else:
                    g_own[q] = piece
        sent = []
        for q in range(pieces):
            over[q].wait()
            h_out[q] = (g_own[q] + g_in[q].astype(F32)).astype(BF16)
            sent.append(push(2 + pieces + q, h_out.at[q], h_in.at[q], far))
            if q == 1:
                swaps, small = rows_done()
        beside = []
        for q in range(pieces):
            sent[q].wait()
            at = cols(c * half + q * size, size)
            whole_out[:, at] = (h_out[q].astype(F32) + h_in[q].astype(F32)).astype(BF16)
            beside.append(push(2 + 2 * pieces + q, whole_out.at[:, at], whole_out.at[:, at], mate))

        for w in range(3):
            for j in range(cuts[w]):
                for k in (1, 2, 3) if mid else (1, 3):
                    weight(w, k, j).wait_send()
                if mid:
                    relay(w, j).wait_send()
                else:
                    second(w, j).wait_send()
                for k in (2, 3) if mid else (1, 2, 3):
                    across(w, k, j).wait_send()
        for i in range(4):
            fetch(i).wait_send()
            for j in range(1, 4):
                spread(i, j).wait_send()
        hid_swap.wait_send()
        for k in range(1, n):
            d_direct(k).wait_send()
        if mid:
            for k in (2, 3):
                d_second(k).wait_send()

        for copy in small:
            copy.wait()
        here = n_own[...]
        for i in range(n - 1):
            here = here + n_in[i]
        there = n_in[n - 1]
        for i in range(n, 2 * n - 1):
            there = there + n_in[i]
        first, later = jnp.where(r == 0, here, there), jnp.where(r == 0, there, here)
        norms[...] = jnp.concatenate(
            [first[:, :sub_e], later[:, :sub_e], first[:, sub_e:], later[:, sub_e:]], axis=1
        )
        for copy in swaps:
            copy.wait()
        for of, theirs in ((True, s_other_m), (False, s_other_e)):
            down_grad[tile(bases[of] + (1 - r) * subs[of], subs[of])] = theirs[...]
        for copy in beside:
            copy.wait()
        input_grad[...] = whole_out[...]

    @pl.when(middle)
    def _():
        body(True)

    @pl.when(~middle)
    def _():
        body(False)


def write_kernel(flow, shard, rows, input_grad, down_grad, norms):
    input_grad[...] = flow[...]
    down_grad[...] = shard[...].astype(F32)
    norms[...] = rows[0]


def split_units(tokens, gate_weight, up_weight, down_weight, out_grad):
    rows, depth = tokens.shape
    width, both = gate_weight.shape
    sub_e = max(both * 13 // 1024, 1) * 16
    sub_m = both // 2 - sub_e
    anywhere = pl.BlockSpec(memory_space=pl.ANY)
    vmem = pl.BlockSpec(memory_space=pltpu.VMEM)
    dma = pltpu.SemaphoreType.DMA
    n, half, pieces = 4, depth // 2, 4
    piece = (pieces, rows, half // pieces)
    peers = 2 * n - 1
    scratch = [((2 * sub_m, depth), BF16)] * 3 + [((2 * sub_e, depth), BF16)] * 3
    scratch += [((2 * rows, depth), BF16), ((4 * rows, depth), BF16)]
    scratch += [((2 * rows, 2 * sub_m), F32)] * 3 + [((2 * rows, 2 * sub_m), BF16)] * 2
    for sub in (sub_m, sub_e):
        scratch += [((4 * rows, sub), BF16), ((2 * rows, sub), BF16)]
    scratch += [((n, sub_m, width), BF16), ((n, sub_e, width), BF16), ((sub_m, width), F32)]
    scratch += [((n, sub_m, width), BF16)] + [((n, sub_e, width), BF16)] * 2
    scratch += [((2, rows, half), BF16)] * 2 + [(piece, F32)] + [(piece, BF16)] * 4
    scratch += [((rows, depth), BF16)] + [((sub_m, width), BF16), ((sub_e, width), BF16)] * 2
    scratch += [((8, both // 2), F32), ((peers, 8, both // 2), F32)]
    input_grad, down_grad, norms = pl.pallas_call(
        block_kernel,
        out_shape=[
            jax.ShapeDtypeStruct((rows, depth), BF16),
            jax.ShapeDtypeStruct((both, width), BF16),
            jax.ShapeDtypeStruct((8, both), F32),
        ],
        in_specs=[anywhere] * 5,
        out_specs=[vmem] * 3,
        scratch_shapes=[pltpu.VMEM(shape, kind) for shape, kind in scratch] + [
            dma((8,)), dma((3, n, 2)), dma((3, n, 2)), dma((3, 2)), dma((3, 2)), dma((3, 2)),
            dma((3, n, 2)), dma((3, n, 2)),
            dma((4, 4)), dma((4, 4)), dma((1,)), dma((1,)),
            dma((n,)), dma((n,)), dma((n,)), dma((n,)),
            dma((2 + 3 * pieces,)), dma((2 + 3 * pieces,)),
            dma((2,)), dma((2,)), dma((peers,)), dma((peers,)),
        ],
        compiler_params=pltpu.CompilerParams(collective_id=0, has_side_effects=True),
        name="block",
    )(gate_weight.T, up_weight.T, down_weight, tokens, out_grad)
    return tuple(pl.pallas_call(
        write_kernel,
        out_shape=[
            jax.ShapeDtypeStruct((rows, depth), BF16),
            jax.ShapeDtypeStruct((both, width), F32),
            jax.ShapeDtypeStruct((both,), F32),
        ],
        in_specs=[vmem] * 3,
        out_specs=[vmem] * 3,
        name="write",
    )(input_grad, down_grad, norms))


def whole_units(tokens, gate_weight, up_weight, down_weight, out_grad):
    down_full = lax.all_gather(down_weight, "fs", axis=1, tiled=True)
    gate_full = lax.all_gather(gate_weight, "fs", axis=0, tiled=True)
    up_full = lax.all_gather(up_weight, "fs", axis=0, tiled=True)
    gate_pre = jnp.dot(tokens, gate_full, preferred_element_type=F32)
    up_pre = jnp.dot(tokens, up_full, preferred_element_type=F32)
    sigma = jax.nn.sigmoid(gate_pre)
    activated = gate_pre * sigma
    hidden = (activated * up_pre).astype(BF16)
    hid_grad = contract_last(out_grad, down_full)
    up_grad = (hid_grad * activated).astype(BF16)
    gate_grad = (hid_grad * up_pre * sigma * (1.0 + gate_pre * (1.0 - sigma))).astype(BF16)
    partial_value = contract_last(gate_grad, gate_full) + contract_last(up_grad, up_full)
    input_grad = lax.psum(partial_value.astype(BF16), "tp")
    columns = lax.all_to_all(out_grad, "fs", split_axis=1, concat_axis=0, tiled=True)
    shard = contract_first(lax.all_gather(hidden, "fs", axis=0, tiled=True), columns)
    shard = lax.psum(shard.astype(BF16), "rep").astype(F32)
    norms = lax.psum(jnp.sum(shard * shard, axis=1), "fs")
    return (input_grad, shard, norms)


def solution(mesh):
    n, rep, tp = mesh.shape["fs"], mesh.shape["rep"], mesh.shape["tp"]

    def on_device(tokens, gate_weight, up_weight, down_weight, out_grad):
        width, both = gate_weight.shape
        if rep == 2 and tp == 4 and n == 4 and both % 32 == 0 and both >= 128 and width % 256 == 0 and tokens.shape[0] % 64 == 0:
            return split_units(tokens, gate_weight, up_weight, down_weight, out_grad)
        return whole_units(tokens, gate_weight, up_weight, down_weight, out_grad)

    return jax.shard_map(
        on_device,
        mesh=mesh,
        in_specs=(
            P(("rep", "fs"), None),
            P("fs", "tp"),
            P("fs", "tp"),
            P("tp", "fs"),
            P(("rep", "fs"), None),
        ),
        out_specs=(P(("rep", "fs"), None), P("tp", "fs"), P("tp")),
        check_vma=False,
    )
```

```python
import jax
import jax.numpy as jnp
from jax import lax
from jax.experimental import pallas as pl
from jax.experimental.pallas import tpu as pltpu
from jax.sharding import PartitionSpec as P

MESH = pl.DeviceIdType.MESH
BF16 = jnp.bfloat16
F32 = jnp.float32


def contract_last(left, right):
    return lax.dot_general(left, right, (((1,), (1,)), ((), ())), preferred_element_type=F32)


def contract_first(left, right):
    return lax.dot_general(left, right, (((0,), (0,)), ((), ())), preferred_element_type=F32)


def block_kernel(
    gate, up, down, tokens, grad, input_grad, down_grad, norms,
    gate_m, up_m, down_m, gate_e, up_e, down_e, tokens_all, grad_all,
    gate_pre, up_pre, hid, gate_grad, up_grad, hid_all_m, hid_out_m, hid_all_e, hid_out_e,
    part_m, part_e, part_own, d_in_m, d_in_e, d_pass,
    f_out, f_in, g_own, g_out, g_in, h_out, h_in, whole_out, s_own_m, s_own_e, s_other_m, s_other_e,
    n_own, n_in, n_sum,
    own_sem, w_send, w_recv, w_pass, b_send, b_recv, y_send, y_recv, t_send, t_recv, hid_send, hid_recv,
    d_send, d_recv, e_send, e_recv, g_send, g_recv, s_send, s_recv, n_send, n_recv, out_sem,
):
    n = 4
    f = lax.axis_index("fs")
    r = lax.axis_index("rep")
    t = lax.axis_index("tp")
    c, x = lax.rem(t, 2), t // 2
    middle = (f == 1) | (f == 2)
    mate, far, pair = {"tp": x * 2 + 1 - c}, {"tp": (1 - x) * 2 + c}, {"rep": 1 - r}
    other = (f, f + 1 - 2 * lax.rem(f, 2), lax.rem(f + 2, n), n - 1 - f)
    rows, depth = tokens.shape
    width = gate.shape[1]
    half, quarter = depth // 2, rows // 4
    pieces = g_out.shape[0]
    size = half // pieces
    owns = (gate, up, down)
    sub_m, sub_e = hid_out_m.shape[1], hid_out_e.shape[1]
    subs = {True: sub_m, False: sub_e}
    bases = {True: 2 * sub_e, False: 0}
    wholes = {True: (gate_m, up_m, down_m), False: (gate_e, up_e, down_e)}

    def cols(start, size):
        return pl.ds(pl.multiple_of(start, size), size)

    def tile(start, size):
        return pl.ds(pl.multiple_of(start, 16), size)

    def remote(src, dst, send, recv, peer):
        return pltpu.make_async_remote_copy(
            src_ref=src, dst_ref=dst, send_sem=send, recv_sem=recv,
            device_id=peer, device_id_type=MESH,
        )

    held = [
        pltpu.make_async_copy(own, whole.at[pl.ds(0, rows)], own_sem.at[i])
        for i, (own, whole) in enumerate(((tokens, tokens_all), (grad, grad_all)))
    ]

    def own_rows(mid):
        sub = subs[mid]
        return [
            pltpu.make_async_copy(
                own.at[tile(bases[mid] + (r if b == 0 else 1 - r) * sub, sub)],
                whole.at[pl.ds(b * sub, sub), cols(f * width, width)],
                own_sem.at[2 + w],
            )
            for w, (own, whole) in enumerate(zip(owns, wholes[mid])) for b in range(2)
        ]

    for copy in held:
        copy.start()

    barrier = pltpu.get_barrier_semaphore()
    peers = [{"rep": lax.rem(r + a, 2), "fs": other[k]}
             for a in range(2) for k in range(n) if a or k]
    for peer in peers + [mate, far]:
        pl.semaphore_signal(barrier, inc=1, device_id=peer, device_id_type=MESH)
    pl.semaphore_wait(barrier, 2 * n + 1)

    cuts = (1, 1, 4)

    def slot(w, k, j):
        return w * 3 + (k - 1) * cuts[w] + j

    def place(w, k, j):
        size = width if j is None else width // cuts[w]
        return cols(other[k] * width + (0 if j is None else j * size), size)

    flows = ((tokens, tokens_all, 1), (grad, grad_all, 1), (grad, grad_all, 2), (grad, grad_all, 3))

    def span(i, q):
        return flows[i][1].at[tile(flows[i][2] * rows + q * quarter, quarter)]

    q_near, q_far = t, (1 - x) * 2 + c

    def fetch(i):
        own = grad_all.at[tile(rows + t * quarter, quarter)] if i == 3 else (
            flows[i][0].at[tile(t * quarter, quarter)])
        return remote(own, span(i, q_near), t_send.at[0], t_recv.at[i],
                      {"fs": other[1]} if i < 2 else pair)

    def spread(i, j):
        q = q_near if j < 3 else q_far
        return remote(span(i, q), span(i, q), t_send.at[0], t_recv.at[(4 if j == 1 else 8) + i],
                      far if j == 1 else mate)

    def hand(i):
        fetch(i).wait_recv()
        spread(i, 1).start()
        spread(i, 2).start()

    def pass_on(i):
        spread(i, 1).wait_recv()
        spread(i, 3).start()

    def complete(i):
        both_quarters = flows[i][1].at[pl.ds(0, 2 * quarter)]
        remote(both_quarters, both_quarters, t_send.at[0], t_recv.at[8 + i], mate).wait_recv()

    def body(mid):
        sub = subs[mid]
        units = 2 * sub
        whole = wholes[mid]
        hid_all, hid_out, part = (hid_all_m, hid_out_m, part_m) if mid else (hid_all_e, hid_out_e, part_e)
        role = (mid, not mid, not mid, mid)
        for copy in own_rows(mid):
            copy.start()

        def strip(w, j):
            size = width // cuts[w]
            return pl.ds(0, width) if j is None else pl.ds(j * size, size)

        def weight(w, k, j, out=True):
            to = role[k] if out else mid
            return remote(
                owns[w].at[tile(bases[to] + r * subs[to], subs[to]), strip(w, j)],
                wholes[to][w].at[pl.ds(0, subs[to]), place(w, 0 if out else k, j)],
                w_send.at[3 * w + k - 1], w_recv.at[slot(w, k, j or 0)], {"fs": other[k]},
            )

        def second(w, j):
            return remote(
                owns[w].at[tile(bases[True] + (1 - r) * sub_m, sub_m), strip(w, j)],
                wholes[True][w].at[pl.ds(sub_m, sub_m), place(w, 1 if mid else 0, j)],
                b_send.at[w], b_recv.at[w], {"fs": other[1]},
            )

        def relay(w, j):
            held_rows = whole[w].at[pl.ds(0, sub), place(w, 1, j)]
            return remote(held_rows, held_rows, w_pass.at[w], w_recv.at[slot(w, 2, j or 0)], {"fs": other[3]})

        def across(w, k, j):
            return remote(
                whole[w].at[pl.ds(0, sub), place(w, k, j)], whole[w].at[pl.ds(sub, sub), place(w, k, j)],
                y_send.at[3 * w + k - 1], y_recv.at[3 * w + k - 1], pair,
            )

        def give(w, k):
            for j in range(cuts[w]):
                weight(w, k, j).start()

        def give_second(w):
            for j in range(cuts[w]):
                second(w, j).start()

        def arrive(w, k):
            for j in range(cuts[w]):
                weight(w, k, j, False).wait_recv()
                (relay(w, j) if mid and k == 1 else across(w, k, j)).start()

        def arrived(w, k):
            if mid and k == 1:
                second(w, None).wait_recv()
            else:
                across(w, k, None).wait_recv()

        def pre(k):
            at = place(0, k, 0)
            for w, target in ((0, gate_pre), (1, up_pre)):
                if k:
                    arrived(w, k)
                product = contract_last(tokens_all[:, at], whole[w][pl.ds(0, units), at])
                if k == 0:
                    target[:, :units] = product
                else:
                    target[:, :units] += product

        def start_pre():
            for copy in held:
                copy.wait()
            for w in range(3):
                mine = whole[w].at[pl.ds(0, units), place(w, 0, None)]
                pltpu.make_async_copy(mine, mine, own_sem.at[2 + w]).wait()
            complete(0)
            pre(0)

        hid_swap = remote(hid_out, hid_all.at[pl.ds(2 * rows, 2 * rows)],
                          hid_send.at[0], hid_recv.at[0], pair)

        def activate():
            gated, raw = gate_pre[:, :units], up_pre[:, :units]
            sigma = jax.nn.sigmoid(gated)
            hidden = (gated * sigma * raw).astype(BF16)
            hid_out[...] = hidden[:, sub:]
            hid_all[pl.ds(0, 2 * rows)] = hidden[:, :sub]
            gate_pre[:, :units] = gated * sigma
            up_pre[:, :units] = raw * sigma * (1.0 + gated * (1.0 - sigma))

        def add_hid(k):
            if k:
                arrived(2, k)
            else:
                complete(1)
            at = cols(other[k] * width, width)
            product = contract_last(grad_all[pl.ds(0, 2 * rows), at], down_rows(at))
            if k == 0:
                hid[:, :units] = product
            else:
                hid[:, :units] += product

        def down_rows(at):
            return whole[2][pl.ds(0, units), at]

        def d_in(k, of):
            return (d_in_m if of else d_in_e).at[k]

        def d_direct(k):
            return remote(part.at[k], d_in(k, mid), d_send.at[0], d_recv.at[k - 1], {"fs": other[k]})

        def d_done(k):
            return remote(d_in(k, role[k]), d_in(k, role[k]), d_send.at[0], d_recv.at[k - 1], {"fs": other[k]})

        def d_first(k):
            return remote(part_e.at[k], d_pass.at[k], d_send.at[0], e_recv.at[k - 2], {"fs": other[1]})

        def d_second(k):
            return remote(d_pass.at[k], d_in(k, False), e_send.at[0], d_recv.at[k - 1], {"fs": other[5 - k]})

        def products():
            complete(2)
            complete(3)
            hid_swap.wait_recv()
            for k in (2, 3, 1, 0):
                at = cols(other[k] * width, width)
                product = contract_first(hid_all[...], grad_all[:, at])
                if k == 0:
                    part_own[pl.ds(0, sub)] = product
                    continue
                part[k] = product.astype(BF16)
                (d_direct if mid or k == 1 else d_first)(k).start()

        def hand_products():
            for k in (2, 3):
                d_first(k).wait_recv()
                d_second(k).start()

        def flow(b, at):
            span = pl.ds(b * rows, rows)
            return (
                jnp.dot(gate_grad[span, :units], whole[0][pl.ds(0, units), at],
                        preferred_element_type=F32)
                + jnp.dot(up_grad[span, :units], whole[1][pl.ds(0, units), at],
                          preferred_element_type=F32)
            )

        def push(group, i, src, dst, peer):
            copy = remote(src, dst, g_send.at[group], g_recv.at[i], peer)
            copy.start()
            return copy

        def put(group, src, dst):
            pltpu.make_async_copy(src, dst, out_sem.at[group]).start()

        swaps = [
            remote(own, theirs, s_send.at[i], s_recv.at[i], pair)
            for i, (own, theirs) in enumerate(((s_own_m, s_other_m), (s_own_e, s_other_e)))
        ]
        sums = {}

        def rows_of(of):
            own = s_own_m if of else s_own_e
            if of == mid:
                d_done(3).wait_recv()
                own[...] = (part_own[pl.ds(0, sub)] + d_in(3, mid)[...].astype(F32)).astype(BF16)
            else:
                d_done(1).wait_recv()
                d_done(2).wait_recv()
                own[...] = (d_in(1, of)[...].astype(F32) + d_in(2, of)[...].astype(F32)).astype(BF16)
            kept = own[...].astype(F32)
            put(1, own, down_grad.at[tile(bases[of] + r * subs[of], subs[of])])
            sums[of] = lax.dot_general(
                jnp.ones((8, width), F32), kept * kept, (((1,), (1,)), ((), ())),
                precision=lax.Precision.HIGHEST, preferred_element_type=F32,
            )

        def rows_done():
            rows_of(False)
            n_own[...] = jnp.concatenate([sums[False], sums[True]], axis=1)
            for i, peer in enumerate(peers):
                remote(n_own, n_in.at[i], n_send.at[0], n_recv.at[0], peer).start()
            swaps[1].start()

        def finish_rows():
            remote(n_in, n_in, n_send.at[0], n_recv.at[0], pair).wait_recv()
            here = n_own[...]
            for i in range(n - 1):
                here = here + n_in[i]
            there = n_in[n - 1]
            for i in range(n, 2 * n - 1):
                there = there + n_in[i]
            first, later = jnp.where(r == 0, here, there), jnp.where(r == 0, there, here)
            n_sum[...] = jnp.concatenate(
                [first[:, :sub_e], later[:, :sub_e], first[:, sub_e:], later[:, sub_e:]], axis=1
            )
            put(2, n_sum, norms)
            for copy in swaps:
                copy.wait_recv()
            for of, theirs in ((True, s_other_m), (False, s_other_e)):
                put(1, theirs, down_grad.at[tile(bases[of] + (1 - r) * subs[of], subs[of])])

        if mid:
            fetch(2).start()
            fetch(0).start()
            give(0, 3)
            give(1, 3)
            give(0, 1)
            fetch(1).start()
            give(1, 1)
            arrive(0, 1)
            give(0, 2)
            arrive(0, 3)
            hand(0)
            arrive(1, 3)
            hand(2)
            arrive(1, 1)
            give(1, 2)
            for k in (1, 3, 2):
                give(2, k)
            pass_on(0)
            arrive(0, 2)
            start_pre()
            hand(1)
            fetch(3).start()
            pass_on(2)
            pre(3)
            arrive(1, 2)
            pass_on(1)
            hand(3)
            arrive(2, 3)
            pre(2)
            pre(1)
            activate()
            hid_swap.start()
            pass_on(3)
            arrive(2, 1)
            add_hid(0)
            add_hid(3)
            arrive(2, 2)
            products()
            add_hid(1)
            add_hid(2)
        else:
            fetch(2).start()
            give(0, 1)
            fetch(0).start()
            give(1, 1)
            fetch(1).start()
            give(0, 3)
            give(1, 3)
            give_second(0)
            give_second(1)
            give(2, 1)
            give(2, 3)
            give_second(2)
            hand(2)
            hand(0)
            arrive(0, 1)
            pass_on(2)
            pass_on(0)
            hand(1)
            fetch(3).start()
            arrive(0, 3)
            arrive(0, 2)
            arrive(1, 1)
            arrive(1, 3)
            pass_on(1)
            start_pre()
            arrive(1, 2)
            hand(3)
            pre(1)
            pre(3)
            pass_on(3)
            arrive(2, 1)
            pre(2)
            activate()
            hid_swap.start()
            arrive(2, 2)
            add_hid(0)
            add_hid(1)
            arrive(2, 3)
            products()
            add_hid(2)
            add_hid(3)

        neighbour = {"fs": other[1]}
        cross = {}
        for b in (1, 0):
            at = pl.ds(b * rows, rows)
            up_grad[at, :units] = (hid[at, :units] * gate_pre[at, :units]).astype(BF16)
            gate_grad[at, :units] = (hid[at, :units] * up_pre[at, :units]).astype(BF16)
            f_out[b] = flow(b, cols((1 - c) * half, half)).astype(BF16)
            cross[b] = push(0, b, f_out.at[b], f_in.at[b], mate)
        over = []
        for b in (1, 0):
            kept = flow(b, cols(c * half, half))
            cross[b].wait_recv()
            kept = kept + f_in[b].astype(F32)
            for q in range(pieces):
                piece = kept[:, q * size:(q + 1) * size]
                if b == 1:
                    g_out[q] = piece.astype(BF16)
                    over.append(push(1, 2 + q, g_out.at[q], g_in.at[q], neighbour))
                else:
                    g_own[q] = piece
            if b == 1 and mid:
                hand_products()
        rows_of(True)
        swaps[0].start()
        sent = []
        for q in range(pieces):
            over[q].wait_recv()
            h_out[q] = (g_own[q] + g_in[q].astype(F32)).astype(BF16)
            sent.append(push(2, 2 + pieces + q, h_out.at[q], h_in.at[q], far))
            if q == 1:
                rows_done()
        beside = []
        for q in range(pieces):
            sent[q].wait_recv()
            at = cols(c * half + q * size, size)
            whole_out[:, at] = (h_out[q].astype(F32) + h_in[q].astype(F32)).astype(BF16)
            beside.append(push(3, 2 + 2 * pieces + q, whole_out.at[:, at], whole_out.at[:, at], mate))
            put(0, whole_out.at[:, at], input_grad.at[:, at])
            if q == pieces - 2:
                finish_rows()

        for w in range(3):
            for k in (1, 2, 3) if mid else (1, 3):
                weight(w, k, None).wait_send()
            (relay if mid else second)(w, None).wait_send()
            for k in (2, 3) if mid else (1, 2, 3):
                across(w, k, None).wait_send()

        def sent_all(ref, sem):
            remote(ref, ref, sem, sem, pair).wait_send()

        sent_all(grad_all, t_send.at[0])
        hid_swap.wait_send()
        sent_all(part.at[pl.ds(1, 3)], d_send.at[0])
        if mid:
            sent_all(d_pass.at[pl.ds(2, 2)], e_send.at[0])
        for i, ref in enumerate((f_out, g_out, h_out, whole_out.at[:, pl.ds(0, half)])):
            sent_all(ref, g_send.at[i])
        sent_all(n_in, n_send.at[0])
        for copy in swaps:
            copy.wait_send()

        for q in range(pieces):
            beside[q].wait_recv()
            at = cols((1 - c) * half + q * size, size)
            put(0, whole_out.at[:, at], input_grad.at[:, at])
        for i, (src, dst) in enumerate(((whole_out, input_grad), (down_grad, down_grad), (n_sum, norms))):
            pltpu.make_async_copy(src, dst, out_sem.at[i]).wait()

    @pl.when(middle)
    def _():
        body(True)

    @pl.when(~middle)
    def _():
        body(False)


def write_kernel(flow, shard, rows, input_grad, down_grad, norms):
    input_grad[...] = flow[...]
    down_grad[...] = shard[...].astype(F32)
    norms[...] = rows[0]


def split_units(tokens, gate_weight, up_weight, down_weight, out_grad):
    rows, depth = tokens.shape
    width, both = gate_weight.shape
    sub_e = max(both * 13 // 1024, 1) * 16
    sub_m = both // 2 - sub_e
    anywhere = pl.BlockSpec(memory_space=pl.ANY)
    vmem = pl.BlockSpec(memory_space=pltpu.VMEM)
    dma = pltpu.SemaphoreType.DMA
    n, half, pieces = 4, depth // 2, 4
    piece = (pieces, rows, half // pieces)
    peers = 2 * n - 1
    scratch = [((2 * sub_m, depth), BF16)] * 3 + [((2 * sub_e, depth), BF16)] * 3
    scratch += [((2 * rows, depth), BF16), ((4 * rows, depth), BF16)]
    scratch += [((2 * rows, 2 * sub_m), F32)] * 3 + [((2 * rows, 2 * sub_m), BF16)] * 2
    for sub in (sub_m, sub_e):
        scratch += [((4 * rows, sub), BF16), ((2 * rows, sub), BF16)]
    scratch += [((n, sub_m, width), BF16), ((n, sub_e, width), BF16), ((sub_m, width), F32)]
    scratch += [((n, sub_m, width), BF16)] + [((n, sub_e, width), BF16)] * 2
    scratch += [((2, rows, half), BF16)] * 2 + [(piece, F32)] + [(piece, BF16)] * 4
    scratch += [((rows, depth), BF16)] + [((sub_m, width), BF16), ((sub_e, width), BF16)] * 2
    scratch += [((8, both // 2), F32), ((peers, 8, both // 2), F32), ((8, both), F32)]
    input_grad, down_grad, norms = pl.pallas_call(
        block_kernel,
        out_shape=[
            jax.ShapeDtypeStruct((rows, depth), BF16),
            jax.ShapeDtypeStruct((both, width), BF16),
            jax.ShapeDtypeStruct((8, both), F32),
        ],
        in_specs=[anywhere] * 5,
        out_specs=[anywhere] * 3,
        scratch_shapes=[pltpu.VMEM(shape, kind) for shape, kind in scratch] + [
            dma((count,)) for count in (
                5, 9, 18, 3, 3, 3, 9, 9, 1, 12, 1, 1, 1, 3, 1, 2, 4, 2 + 3 * pieces, 2, 2, 1, 1, 3,
            )
        ],
        compiler_params=pltpu.CompilerParams(collective_id=0, has_side_effects=True),
        name="block",
    )(gate_weight.T, up_weight.T, down_weight, tokens, out_grad)
    return tuple(pl.pallas_call(
        write_kernel,
        out_shape=[
            jax.ShapeDtypeStruct((rows, depth), BF16),
            jax.ShapeDtypeStruct((both, width), F32),
            jax.ShapeDtypeStruct((both,), F32),
        ],
        in_specs=[vmem] * 3,
        out_specs=[vmem] * 3,
        name="write",
    )(input_grad, down_grad, norms))


def whole_units(tokens, gate_weight, up_weight, down_weight, out_grad):
    down_full = lax.all_gather(down_weight, "fs", axis=1, tiled=True)
    gate_full = lax.all_gather(gate_weight, "fs", axis=0, tiled=True)
    up_full = lax.all_gather(up_weight, "fs", axis=0, tiled=True)
    gate_pre = jnp.dot(tokens, gate_full, preferred_element_type=F32)
    up_pre = jnp.dot(tokens, up_full, preferred_element_type=F32)
    sigma = jax.nn.sigmoid(gate_pre)
    activated = gate_pre * sigma
    hidden = (activated * up_pre).astype(BF16)
    hid_grad = contract_last(out_grad, down_full)
    up_grad = (hid_grad * activated).astype(BF16)
    gate_grad = (hid_grad * up_pre * sigma * (1.0 + gate_pre * (1.0 - sigma))).astype(BF16)
    partial_value = contract_last(gate_grad, gate_full) + contract_last(up_grad, up_full)
    input_grad = lax.psum(partial_value.astype(BF16), "tp")
    columns = lax.all_to_all(out_grad, "fs", split_axis=1, concat_axis=0, tiled=True)
    shard = contract_first(lax.all_gather(hidden, "fs", axis=0, tiled=True), columns)
    shard = lax.psum(shard.astype(BF16), "rep").astype(F32)
    norms = lax.psum(jnp.sum(shard * shard, axis=1), "fs")
    return (input_grad, shard, norms)


def solution(mesh):
    n, rep, tp = mesh.shape["fs"], mesh.shape["rep"], mesh.shape["tp"]

    def on_device(tokens, gate_weight, up_weight, down_weight, out_grad):
        width, both = gate_weight.shape
        if rep == 2 and tp == 4 and n == 4 and both % 32 == 0 and both >= 128 and width % 512 == 0 and tokens.shape[0] % 64 == 0:
            return split_units(tokens, gate_weight, up_weight, down_weight, out_grad)
        return whole_units(tokens, gate_weight, up_weight, down_weight, out_grad)

    return jax.shard_map(
        on_device,
        mesh=mesh,
        in_specs=(
            P(("rep", "fs"), None),
            P("fs", "tp"),
            P("fs", "tp"),
            P("tp", "fs"),
            P(("rep", "fs"), None),
        ),
        out_specs=(P(("rep", "fs"), None), P("tp", "fs"), P("tp")),
        check_vma=False,
    )
```

```python
import jax
import jax.numpy as jnp
from jax import lax
from jax.experimental import pallas as pl
from jax.experimental.pallas import tpu as pltpu
from jax.sharding import PartitionSpec as P

MESH = pl.DeviceIdType.MESH
BF16 = jnp.bfloat16
F32 = jnp.float32


def contract_last(left, right):
    return lax.dot_general(left, right, (((1,), (1,)), ((), ())), preferred_element_type=F32)


def contract_first(left, right):
    return lax.dot_general(left, right, (((0,), (0,)), ((), ())), preferred_element_type=F32)


def block_kernel(
    gate, up, down, tokens, grad, input_grad, down_grad, norms,
    gate_m, up_m, down_m, gate_e, up_e, down_e, tokens_all, grad_all,
    gate_pre, up_pre, hid, gate_grad, up_grad, hid_all_m, hid_out_m, hid_all_e, hid_out_e,
    part_m, part_e, part_own, d_in_m, d_in_e, d_pass,
    f_out, f_in, g_own, g_out, g_in, x_out, x_in, h_out, h_in, whole_out, s_own_m, s_own_e, s_other_m, s_other_e,
    n_own, n_in, n_sum,
    own_sem, w_send, w_recv, w_pass, b_send, b_recv, y_send, y_recv, t_send, t_recv, hid_send, hid_recv,
    d_send, d_recv, e_send, e_recv, g_send, g_recv, s_send, s_recv, n_send, n_recv, out_sem,
):
    n = 4
    f = lax.axis_index("fs")
    r = lax.axis_index("rep")
    t = lax.axis_index("tp")
    c, x = lax.rem(t, 2), t // 2
    middle = (f == 1) | (f == 2)
    mate, far, pair = {"tp": x * 2 + 1 - c}, {"tp": (1 - x) * 2 + c}, {"rep": 1 - r}
    other = (f, f + 1 - 2 * lax.rem(f, 2), lax.rem(f + 2, n), n - 1 - f)
    rows, depth = tokens.shape
    width = gate.shape[1]
    half, quarter = depth // 2, rows // 4
    size = g_out.shape[2]
    owns = (gate, up, down)
    sub_m, sub_e = hid_out_m.shape[1], hid_out_e.shape[1]
    subs = {True: sub_m, False: sub_e}
    bases = {True: 2 * sub_e, False: 0}
    wholes = {True: (gate_m, up_m, down_m), False: (gate_e, up_e, down_e)}

    def cols(start, size):
        return pl.ds(pl.multiple_of(start, size), size)

    def tile(start, size):
        return pl.ds(pl.multiple_of(start, 16), size)

    def remote(src, dst, send, recv, peer):
        return pltpu.make_async_remote_copy(
            src_ref=src, dst_ref=dst, send_sem=send, recv_sem=recv,
            device_id=peer, device_id_type=MESH,
        )

    held = [
        pltpu.make_async_copy(own, whole.at[pl.ds(0, rows)], own_sem.at[i])
        for i, (own, whole) in enumerate(((tokens, tokens_all), (grad, grad_all)))
    ]

    def own_rows(mid):
        sub = subs[mid]
        return [
            pltpu.make_async_copy(
                own.at[tile(bases[mid] + (r if b == 0 else 1 - r) * sub, sub)],
                whole.at[pl.ds(b * sub, sub), cols(f * width, width)],
                own_sem.at[2 + w],
            )
            for w, (own, whole) in enumerate(zip(owns, wholes[mid])) for b in range(2)
        ]

    for copy in held:
        copy.start()

    barrier = pltpu.get_barrier_semaphore()
    peers = [{"rep": lax.rem(r + a, 2), "fs": other[k]}
             for a in range(2) for k in range(n) if a or k]
    for peer in peers + [mate, far]:
        pl.semaphore_signal(barrier, inc=1, device_id=peer, device_id_type=MESH)
    pl.semaphore_wait(barrier, 2 * n + 1)

    cuts = (1, 1, 4)

    def slot(w, k, j):
        return w * 3 + (k - 1) * cuts[w] + j

    def place(w, k, j):
        size = width if j is None else width // cuts[w]
        return cols(other[k] * width + (0 if j is None else j * size), size)

    flows = ((tokens, tokens_all, 1), (grad, grad_all, 1), (grad, grad_all, 2), (grad, grad_all, 3))

    def span(i, q):
        return flows[i][1].at[tile(flows[i][2] * rows + q * quarter, quarter)]

    q_near, q_far = t, (1 - x) * 2 + c

    def fetch(i):
        own = grad_all.at[tile(rows + t * quarter, quarter)] if i == 3 else (
            flows[i][0].at[tile(t * quarter, quarter)])
        return remote(own, span(i, q_near), t_send.at[0], t_recv.at[i],
                      {"fs": other[1]} if i < 2 else pair)

    def spread(i, j):
        q = q_near if j < 3 else q_far
        return remote(span(i, q), span(i, q), t_send.at[0], t_recv.at[(4 if j == 1 else 8) + i],
                      far if j == 1 else mate)

    def hand(i):
        fetch(i).wait_recv()
        spread(i, 1).start()
        spread(i, 2).start()

    def pass_on(i):
        spread(i, 1).wait_recv()
        spread(i, 3).start()

    def complete(i):
        both_quarters = flows[i][1].at[pl.ds(0, 2 * quarter)]
        remote(both_quarters, both_quarters, t_send.at[0], t_recv.at[8 + i], mate).wait_recv()

    def body(mid):
        sub = subs[mid]
        units = 2 * sub
        whole = wholes[mid]
        hid_all, hid_out, part = (hid_all_m, hid_out_m, part_m) if mid else (hid_all_e, hid_out_e, part_e)
        role = (mid, not mid, not mid, mid)
        for copy in own_rows(mid):
            copy.start()

        def strip(w, j):
            size = width // cuts[w]
            return pl.ds(0, width) if j is None else pl.ds(j * size, size)

        def weight(w, k, j, out=True):
            to = role[k] if out else mid
            return remote(
                owns[w].at[tile(bases[to] + r * subs[to], subs[to]), strip(w, j)],
                wholes[to][w].at[pl.ds(0, subs[to]), place(w, 0 if out else k, j)],
                w_send.at[3 * w + k - 1], w_recv.at[slot(w, k, j or 0)], {"fs": other[k]},
            )

        def second(w, j):
            return remote(
                owns[w].at[tile(bases[True] + (1 - r) * sub_m, sub_m), strip(w, j)],
                wholes[True][w].at[pl.ds(sub_m, sub_m), place(w, 1 if mid else 0, j)],
                b_send.at[w], b_recv.at[w], {"fs": other[1]},
            )

        def relay(w, j):
            held_rows = whole[w].at[pl.ds(0, sub), place(w, 1, j)]
            return remote(held_rows, held_rows, w_pass.at[w], w_recv.at[slot(w, 2, j or 0)], {"fs": other[3]})

        def across(w, k, j):
            return remote(
                whole[w].at[pl.ds(0, sub), place(w, k, j)], whole[w].at[pl.ds(sub, sub), place(w, k, j)],
                y_send.at[3 * w + k - 1], y_recv.at[3 * w + k - 1], pair,
            )

        def give(w, k):
            for j in range(cuts[w]):
                weight(w, k, j).start()

        def give_second(w):
            for j in range(cuts[w]):
                second(w, j).start()

        def arrive(w, k):
            for j in range(cuts[w]):
                weight(w, k, j, False).wait_recv()
                (relay(w, j) if mid and k == 1 else across(w, k, j)).start()

        def arrived(w, k):
            if mid and k == 1:
                second(w, None).wait_recv()
            else:
                across(w, k, None).wait_recv()

        def pre(k):
            at = place(0, k, 0)
            for w, target in ((0, gate_pre), (1, up_pre)):
                if k:
                    arrived(w, k)
                product = contract_last(tokens_all[:, at], whole[w][pl.ds(0, units), at])
                if k == 0:
                    target[:, :units] = product
                else:
                    target[:, :units] += product

        def start_pre():
            for copy in held:
                copy.wait()
            for w in range(3):
                mine = whole[w].at[pl.ds(0, units), place(w, 0, None)]
                pltpu.make_async_copy(mine, mine, own_sem.at[2 + w]).wait()
            complete(0)
            pre(0)

        hid_swap = remote(hid_out, hid_all.at[pl.ds(2 * rows, 2 * rows)],
                          hid_send.at[0], hid_recv.at[0], pair)

        def activate():
            gated, raw = gate_pre[:, :units], up_pre[:, :units]
            sigma = jax.nn.sigmoid(gated)
            hidden = (gated * sigma * raw).astype(BF16)
            hid_out[...] = hidden[:, sub:]
            hid_all[pl.ds(0, 2 * rows)] = hidden[:, :sub]
            gate_pre[:, :units] = gated * sigma
            up_pre[:, :units] = raw * sigma * (1.0 + gated * (1.0 - sigma))

        def add_hid(k):
            if k:
                arrived(2, k)
            else:
                complete(1)
            at = cols(other[k] * width, width)
            product = contract_last(grad_all[pl.ds(0, 2 * rows), at], down_rows(at))
            if k == 0:
                hid[:, :units] = product
            else:
                hid[:, :units] += product

        def down_rows(at):
            return whole[2][pl.ds(0, units), at]

        def d_in(k, of):
            return (d_in_m if of else d_in_e).at[k]

        def d_direct(k):
            return remote(part.at[k], d_in(k, mid), d_send.at[0], d_recv.at[k - 1], {"fs": other[k]})

        def d_done(k):
            return remote(d_in(k, role[k]), d_in(k, role[k]), d_send.at[0], d_recv.at[k - 1], {"fs": other[k]})

        def d_first(k):
            return remote(part_e.at[k], d_pass.at[k], d_send.at[0], e_recv.at[k - 2], {"fs": other[1]})

        def d_second(k):
            return remote(d_pass.at[k], d_in(k, False), e_send.at[0], d_recv.at[k - 1], {"fs": other[5 - k]})

        def products():
            complete(2)
            complete(3)
            hid_swap.wait_recv()
            for k in (2, 3, 1, 0) if mid else (3, 2, 1, 0):
                at = cols(other[k] * width, width)
                product = contract_first(hid_all[...], grad_all[:, at])
                if k == 0:
                    part_own[pl.ds(0, sub)] = product
                    continue
                part[k] = product.astype(BF16)
                (d_direct if mid or k == 1 else d_first)(k).start()

        def hand_products():
            for k in (3, 2):
                d_first(k).wait_recv()
                d_second(k).start()

        def flow(b, at):
            span = pl.ds(b * rows, rows)
            return (
                jnp.dot(gate_grad[span, :units], whole[0][pl.ds(0, units), at],
                        preferred_element_type=F32)
                + jnp.dot(up_grad[span, :units], whole[1][pl.ds(0, units), at],
                          preferred_element_type=F32)
            )

        def push(group, i, src, dst, peer):
            copy = remote(src, dst, g_send.at[group], g_recv.at[i], peer)
            copy.start()
            return copy

        def put(group, src, dst):
            pltpu.make_async_copy(src, dst, out_sem.at[group]).start()

        swaps = [
            remote(own, theirs, s_send.at[i], s_recv.at[i], pair)
            for i, (own, theirs) in enumerate(((s_own_m, s_other_m), (s_own_e, s_other_e)))
        ]
        sums = {}

        def rows_of(of):
            own = s_own_m if of else s_own_e
            if of == mid:
                d_done(3).wait_recv()
                own[...] = (part_own[pl.ds(0, sub)] + d_in(3, mid)[...].astype(F32)).astype(BF16)
            else:
                d_done(1).wait_recv()
                d_done(2).wait_recv()
                own[...] = (d_in(1, of)[...].astype(F32) + d_in(2, of)[...].astype(F32)).astype(BF16)
            kept = own[...].astype(F32)
            put(1, own, down_grad.at[tile(bases[of] + r * subs[of], subs[of])])
            sums[of] = lax.dot_general(
                jnp.ones((8, width), F32), kept * kept, (((1,), (1,)), ((), ())),
                precision=lax.Precision.HIGHEST, preferred_element_type=F32,
            )

        def rows_done():
            rows_of(False)
            n_own[...] = jnp.concatenate([sums[False], sums[True]], axis=1)
            for i, peer in enumerate(peers):
                remote(n_own, n_in.at[i], n_send.at[0], n_recv.at[0], peer).start()
            swaps[1].start()

        def finish_rows():
            remote(n_in, n_in, n_send.at[0], n_recv.at[0], pair).wait_recv()
            here = n_own[...]
            for i in range(n - 1):
                here = here + n_in[i]
            there = n_in[n - 1]
            for i in range(n, 2 * n - 1):
                there = there + n_in[i]
            first, later = jnp.where(r == 0, here, there), jnp.where(r == 0, there, here)
            n_sum[...] = jnp.concatenate(
                [first[:, :sub_e], later[:, :sub_e], first[:, sub_e:], later[:, sub_e:]], axis=1
            )
            put(2, n_sum, norms)
            for copy in swaps:
                copy.wait_recv()
            for of, theirs in ((True, s_other_m), (False, s_other_e)):
                put(1, theirs, down_grad.at[tile(bases[of] + (1 - r) * subs[of], subs[of])])

        if mid:
            fetch(2).start()
            fetch(0).start()
            give(0, 3)
            give(1, 3)
            give(0, 1)
            fetch(1).start()
            give(1, 1)
            arrive(0, 1)
            give(0, 2)
            arrive(0, 3)
            hand(0)
            arrive(1, 3)
            hand(2)
            arrive(1, 1)
            give(1, 2)
            for k in (1, 3, 2):
                give(2, k)
            pass_on(0)
            arrive(0, 2)
            start_pre()
            hand(1)
            fetch(3).start()
            pass_on(2)
            pre(3)
            arrive(1, 2)
            pass_on(1)
            hand(3)
            arrive(2, 3)
            pre(2)
            pre(1)
            activate()
            hid_swap.start()
            pass_on(3)
            arrive(2, 1)
            add_hid(0)
            add_hid(3)
            arrive(2, 2)
            products()
            add_hid(1)
            add_hid(2)
        else:
            fetch(2).start()
            give(0, 1)
            fetch(0).start()
            give(1, 1)
            fetch(1).start()
            give(0, 3)
            give(1, 3)
            give_second(0)
            give_second(1)
            give(2, 1)
            give(2, 3)
            give_second(2)
            hand(2)
            hand(0)
            arrive(0, 1)
            pass_on(2)
            pass_on(0)
            hand(1)
            fetch(3).start()
            arrive(0, 3)
            arrive(0, 2)
            arrive(1, 1)
            arrive(1, 3)
            pass_on(1)
            start_pre()
            arrive(1, 2)
            hand(3)
            pre(1)
            pre(3)
            pass_on(3)
            arrive(2, 1)
            pre(2)
            activate()
            hid_swap.start()
            arrive(2, 2)
            add_hid(0)
            add_hid(1)
            arrive(2, 3)
            products()
            add_hid(2)
            add_hid(3)

        neighbour = {"fs": other[1]}
        cross = {}
        for b in (1, 0):
            at = pl.ds(b * rows, rows)
            up_grad[at, :units] = (hid[at, :units] * gate_pre[at, :units]).astype(BF16)
            gate_grad[at, :units] = (hid[at, :units] * up_pre[at, :units]).astype(BF16)
            f_out[b] = flow(b, cols((1 - c) * half, half)).astype(BF16)
            cross[b] = push(0, b, f_out.at[b], f_in.at[b], mate)
        mine, theirs = 2 + x, 3 - x

        def lanes(q, core=c):
            return cols(core * half + q * size, size)

        def piece(b, q):
            return flow(b, lanes(q)) + f_in[b, :, cols(q * size, size)].astype(F32)

        reduced, over = {}, []
        for b in (1, 0):
            first = flow(b, lanes(theirs))
            cross[b].wait_recv()
            x_out[b] = (first + f_in[b, :, cols(theirs * size, size)].astype(F32)).astype(BF16)
            reduced[b] = push(2, 5 + b, x_out.at[b], x_in.at[b], far)
            for q in range(2):
                if b == 1:
                    g_out[q] = piece(b, q).astype(BF16)
                    over.append(push(1, 2 + q, g_out.at[q], g_in.at[q], neighbour))
                else:
                    g_own[q] = piece(b, q)
            g_own[2 + b] = piece(b, mine)
        reduced[1].wait_recv()
        g_out[2] = (g_own[3] + x_in[1].astype(F32)).astype(BF16)
        over.append(push(1, 4, g_out.at[2], g_in.at[2], neighbour))
        if mid:
            hand_products()
        reduced[0].wait_recv()
        g_own[2] += x_in[0].astype(F32)
        sent = []
        for q in range(2):
            over[q].wait_recv()
            h_out[q] = (g_own[q] + g_in[q].astype(F32)).astype(BF16)
            sent.append(push(3, 7 + q, h_out.at[q], h_in.at[q], far))
            if q == 0:
                rows_of(True)
                swaps[0].start()
        if not mid:
            rows_done()
        beside = {}

        def finish(i, q):
            part_out = whole_out.at[:, lanes(q)]
            beside[i] = push(4, 10 + i, part_out, part_out, mate)
            put(0, part_out, input_grad.at[:, lanes(q)])

        over[2].wait_recv()
        whole_out[:, lanes(mine)] = (g_own[2] + g_in[2].astype(F32)).astype(BF16)
        gathered = push(5, 9, whole_out.at[:, lanes(mine)], whole_out.at[:, lanes(mine)], far)
        finish(2, mine)
        if mid:
            rows_done()
        for q in range(2):
            sent[q].wait_recv()
            whole_out[:, lanes(q)] = (h_out[q].astype(F32) + h_in[q].astype(F32)).astype(BF16)
            finish(q, q)
        finish_rows()
        gathered.wait_recv()
        finish(3, theirs)

        for w in range(3):
            for k in (1, 2, 3) if mid else (1, 3):
                weight(w, k, None).wait_send()
            (relay if mid else second)(w, None).wait_send()
            for k in (2, 3) if mid else (1, 2, 3):
                across(w, k, None).wait_send()

        def sent_all(ref, sem):
            remote(ref, ref, sem, sem, pair).wait_send()

        sent_all(grad_all, t_send.at[0])
        hid_swap.wait_send()
        sent_all(part.at[pl.ds(1, 3)], d_send.at[0])
        if mid:
            sent_all(d_pass.at[pl.ds(2, 2)], e_send.at[0])
        for i, ref in enumerate((
            f_out, g_out, x_out, h_out, whole_out.at[:, pl.ds(0, half)], whole_out.at[:, pl.ds(0, size)],
        )):
            sent_all(ref, g_send.at[i])
        sent_all(n_in, n_send.at[0])
        for copy in swaps:
            copy.wait_send()

        for i, q in ((2, mine), (0, 0), (1, 1), (3, theirs)):
            beside[i].wait_recv()
            part_in = lanes(q, 1 - c)
            put(0, whole_out.at[:, part_in], input_grad.at[:, part_in])
        for i, (src, dst) in enumerate(((whole_out, input_grad), (down_grad, down_grad), (n_sum, norms))):
            pltpu.make_async_copy(src, dst, out_sem.at[i]).wait()

    @pl.when(middle)
    def _():
        body(True)

    @pl.when(~middle)
    def _():
        body(False)


def write_kernel(flow, shard, rows, input_grad, down_grad, norms):
    input_grad[...] = flow[...]
    down_grad[...] = shard[...].astype(F32)
    norms[...] = rows[0]


def split_units(tokens, gate_weight, up_weight, down_weight, out_grad):
    rows, depth = tokens.shape
    width, both = gate_weight.shape
    sub_e = max(both * 13 // 1024, 1) * 16
    sub_m = both // 2 - sub_e
    anywhere = pl.BlockSpec(memory_space=pl.ANY)
    vmem = pl.BlockSpec(memory_space=pltpu.VMEM)
    dma = pltpu.SemaphoreType.DMA
    n, half, size = 4, depth // 2, depth // 8
    peers = 2 * n - 1
    scratch = [((2 * sub_m, depth), BF16)] * 3 + [((2 * sub_e, depth), BF16)] * 3
    scratch += [((2 * rows, depth), BF16), ((4 * rows, depth), BF16)]
    scratch += [((2 * rows, 2 * sub_m), F32)] * 3 + [((2 * rows, 2 * sub_m), BF16)] * 2
    for sub in (sub_m, sub_e):
        scratch += [((4 * rows, sub), BF16), ((2 * rows, sub), BF16)]
    scratch += [((n, sub_m, width), BF16), ((n, sub_e, width), BF16), ((sub_m, width), F32)]
    scratch += [((n, sub_m, width), BF16)] + [((n, sub_e, width), BF16)] * 2
    scratch += [((2, rows, half), BF16)] * 2 + [((4, rows, size), F32)]
    scratch += [((3, rows, size), BF16)] * 2 + [((2, rows, size), BF16)] * 4
    scratch += [((rows, depth), BF16)] + [((sub_m, width), BF16), ((sub_e, width), BF16)] * 2
    scratch += [((8, both // 2), F32), ((peers, 8, both // 2), F32), ((8, both), F32)]
    input_grad, down_grad, norms = pl.pallas_call(
        block_kernel,
        out_shape=[
            jax.ShapeDtypeStruct((rows, depth), BF16),
            jax.ShapeDtypeStruct((both, width), BF16),
            jax.ShapeDtypeStruct((8, both), F32),
        ],
        in_specs=[anywhere] * 5,
        out_specs=[anywhere] * 3,
        scratch_shapes=[pltpu.VMEM(shape, kind) for shape, kind in scratch] + [
            dma((count,)) for count in (
                5, 9, 18, 3, 3, 3, 9, 9, 1, 12, 1, 1, 1, 3, 1, 2, 6, 14, 2, 2, 1, 1, 3,
            )
        ],
        compiler_params=pltpu.CompilerParams(collective_id=0, has_side_effects=True),
        name="block",
    )(gate_weight.T, up_weight.T, down_weight, tokens, out_grad)
    return tuple(pl.pallas_call(
        write_kernel,
        out_shape=[
            jax.ShapeDtypeStruct((rows, depth), BF16),
            jax.ShapeDtypeStruct((both, width), F32),
            jax.ShapeDtypeStruct((both,), F32),
        ],
        in_specs=[vmem] * 3,
        out_specs=[vmem] * 3,
        name="write",
    )(input_grad, down_grad, norms))


def whole_units(tokens, gate_weight, up_weight, down_weight, out_grad):
    down_full = lax.all_gather(down_weight, "fs", axis=1, tiled=True)
    gate_full = lax.all_gather(gate_weight, "fs", axis=0, tiled=True)
    up_full = lax.all_gather(up_weight, "fs", axis=0, tiled=True)
    gate_pre = jnp.dot(tokens, gate_full, preferred_element_type=F32)
    up_pre = jnp.dot(tokens, up_full, preferred_element_type=F32)
    sigma = jax.nn.sigmoid(gate_pre)
    activated = gate_pre * sigma
    hidden = (activated * up_pre).astype(BF16)
    hid_grad = contract_last(out_grad, down_full)
    up_grad = (hid_grad * activated).astype(BF16)
    gate_grad = (hid_grad * up_pre * sigma * (1.0 + gate_pre * (1.0 - sigma))).astype(BF16)
    partial_value = contract_last(gate_grad, gate_full) + contract_last(up_grad, up_full)
    input_grad = lax.psum(partial_value.astype(BF16), "tp")
    columns = lax.all_to_all(out_grad, "fs", split_axis=1, concat_axis=0, tiled=True)
    shard = contract_first(lax.all_gather(hidden, "fs", axis=0, tiled=True), columns)
    shard = lax.psum(shard.astype(BF16), "rep").astype(F32)
    norms = lax.psum(jnp.sum(shard * shard, axis=1), "fs")
    return (input_grad, shard, norms)


def solution(mesh):
    n, rep, tp = mesh.shape["fs"], mesh.shape["rep"], mesh.shape["tp"]

    def on_device(tokens, gate_weight, up_weight, down_weight, out_grad):
        width, both = gate_weight.shape
        if rep == 2 and tp == 4 and n == 4 and both % 32 == 0 and both >= 128 and width % 512 == 0 and tokens.shape[0] % 64 == 0:
            return split_units(tokens, gate_weight, up_weight, down_weight, out_grad)
        return whole_units(tokens, gate_weight, up_weight, down_weight, out_grad)

    return jax.shard_map(
        on_device,
        mesh=mesh,
        in_specs=(
            P(("rep", "fs"), None),
            P("fs", "tp"),
            P("fs", "tp"),
            P("tp", "fs"),
            P(("rep", "fs"), None),
        ),
        out_specs=(P(("rep", "fs"), None), P("tp", "fs"), P("tp")),
        check_vma=False,
    )
```

```python
import jax
import jax.numpy as jnp
from jax import lax
from jax.experimental import pallas as pl
from jax.experimental.pallas import tpu as pltpu
from jax.sharding import PartitionSpec as P

MESH = pl.DeviceIdType.MESH
BF16 = jnp.bfloat16
F32 = jnp.float32


def contract_last(left, right):
    return lax.dot_general(left, right, (((1,), (1,)), ((), ())), preferred_element_type=F32)


def contract_first(left, right):
    return lax.dot_general(left, right, (((0,), (0,)), ((), ())), preferred_element_type=F32)


def block_kernel(
    gate, up, down, tokens, grad, input_grad, down_grad, norms,
    gate_m, up_m, down_m, gate_e, up_e, down_e, tokens_all, grad_all,
    gate_pre, up_pre, hid, gate_grad, up_grad, hid_all_m, hid_out_m, hid_all_e, hid_out_e,
    part_m, part_e, part_own, d_in_m, d_in_e, d_pass,
    f_out, f_in, g_own, g_out, g_in, x_out, x_in, h_out, h_in, whole_out, s_own_m, s_own_e,
    n_own, n_in, n_sum,
    own_sem, w_send, w_recv, w_pass, b_send, b_recv, y_send, y_recv, t_send, t_recv, hid_send, hid_recv,
    d_send, d_recv, e_send, e_recv, g_send, g_recv, s_send, s_recv, n_send, n_recv, out_sem,
):
    n = 4
    f = lax.axis_index("fs")
    r = lax.axis_index("rep")
    t = lax.axis_index("tp")
    c, x = lax.rem(t, 2), t // 2
    middle = (f == 1) | (f == 2)
    mate, far, pair = {"tp": x * 2 + 1 - c}, {"tp": (1 - x) * 2 + c}, {"rep": 1 - r}
    other = (f, f + 1 - 2 * lax.rem(f, 2), lax.rem(f + 2, n), n - 1 - f)
    rows, depth = tokens.shape
    width = gate.shape[1]
    half, quarter = depth // 2, rows // 4
    size = g_out.shape[2]
    owns = (gate, up, down)
    sub_m, sub_e = hid_out_m.shape[1], hid_out_e.shape[1]
    subs = {True: sub_m, False: sub_e}
    bases = {True: 2 * sub_e, False: 0}
    wholes = {True: (gate_m, up_m, down_m), False: (gate_e, up_e, down_e)}

    def cols(start, size):
        return pl.ds(pl.multiple_of(start, size), size)

    def tile(start, size):
        return pl.ds(pl.multiple_of(start, 16), size)

    def remote(src, dst, send, recv, peer):
        return pltpu.make_async_remote_copy(
            src_ref=src, dst_ref=dst, send_sem=send, recv_sem=recv,
            device_id=peer, device_id_type=MESH,
        )

    held = [
        pltpu.make_async_copy(own, whole.at[pl.ds(0, rows)], own_sem.at[i])
        for i, (own, whole) in enumerate(((tokens, tokens_all), (grad, grad_all)))
    ]

    def own_rows(mid):
        sub = subs[mid]
        return [
            pltpu.make_async_copy(
                own.at[tile(bases[mid] + (r if b == 0 else 1 - r) * sub, sub)],
                whole.at[pl.ds(b * sub, sub), cols(f * width, width)],
                own_sem.at[2 + w],
            )
            for w, (own, whole) in enumerate(zip(owns, wholes[mid])) for b in range(2)
        ]

    for copy in held:
        copy.start()

    barrier = pltpu.get_barrier_semaphore()
    peers = [{"rep": lax.rem(r + a, 2), "fs": other[k]}
             for a in range(2) for k in range(n) if a or k]
    for peer in peers + [mate, far]:
        pl.semaphore_signal(barrier, inc=1, device_id=peer, device_id_type=MESH)
    pl.semaphore_wait(barrier, 2 * n + 1)

    cuts = (1, 1, 4)

    def slot(w, k, j):
        return w * 3 + (k - 1) * cuts[w] + j

    def place(w, k, j):
        size = width if j is None else width // cuts[w]
        return cols(other[k] * width + (0 if j is None else j * size), size)

    flows = ((tokens, tokens_all, 1), (grad, grad_all, 1), (grad, grad_all, 2), (grad, grad_all, 3))

    def span(i, q):
        return flows[i][1].at[tile(flows[i][2] * rows + q * quarter, quarter)]

    q_near, q_far = t, (1 - x) * 2 + c

    def fetch(i):
        own = grad_all.at[tile(rows + t * quarter, quarter)] if i == 3 else (
            flows[i][0].at[tile(t * quarter, quarter)])
        return remote(own, span(i, q_near), t_send.at[0], t_recv.at[i],
                      {"fs": other[1]} if i < 2 else pair)

    def spread(i, j):
        q = q_near if j < 3 else q_far
        return remote(span(i, q), span(i, q), t_send.at[0], t_recv.at[(4 if j == 1 else 8) + i],
                      far if j == 1 else mate)

    def hand(i):
        fetch(i).wait_recv()
        spread(i, 1).start()
        spread(i, 2).start()

    def pass_on(i):
        spread(i, 1).wait_recv()
        spread(i, 3).start()

    def complete(i):
        both_quarters = flows[i][1].at[pl.ds(0, 2 * quarter)]
        remote(both_quarters, both_quarters, t_send.at[0], t_recv.at[8 + i], mate).wait_recv()

    def body(mid):
        sub = subs[mid]
        units = 2 * sub
        whole = wholes[mid]
        hid_all, hid_out, part = (hid_all_m, hid_out_m, part_m) if mid else (hid_all_e, hid_out_e, part_e)
        role = (mid, not mid, not mid, mid)
        for copy in own_rows(mid):
            copy.start()

        def strip(w, j):
            size = width // cuts[w]
            return pl.ds(0, width) if j is None else pl.ds(j * size, size)

        def weight(w, k, j, out=True):
            to = role[k] if out else mid
            return remote(
                owns[w].at[tile(bases[to] + r * subs[to], subs[to]), strip(w, j)],
                wholes[to][w].at[pl.ds(0, subs[to]), place(w, 0 if out else k, j)],
                w_send.at[3 * w + k - 1], w_recv.at[slot(w, k, j or 0)], {"fs": other[k]},
            )

        def second(w, j):
            return remote(
                owns[w].at[tile(bases[True] + (1 - r) * sub_m, sub_m), strip(w, j)],
                wholes[True][w].at[pl.ds(sub_m, sub_m), place(w, 1 if mid else 0, j)],
                b_send.at[w], b_recv.at[w], {"fs": other[1]},
            )

        def relay(w, j):
            held_rows = whole[w].at[pl.ds(0, sub), place(w, 1, j)]
            return remote(held_rows, held_rows, w_pass.at[w], w_recv.at[slot(w, 2, j or 0)], {"fs": other[3]})

        def across(w, k, j):
            return remote(
                whole[w].at[pl.ds(0, sub), place(w, k, j)], whole[w].at[pl.ds(sub, sub), place(w, k, j)],
                y_send.at[3 * w + k - 1], y_recv.at[3 * w + k - 1], pair,
            )

        def give(w, k):
            for j in range(cuts[w]):
                weight(w, k, j).start()

        def give_second(w):
            for j in range(cuts[w]):
                second(w, j).start()

        def arrive(w, k):
            for j in range(cuts[w]):
                weight(w, k, j, False).wait_recv()
                (relay(w, j) if mid and k == 1 else across(w, k, j)).start()

        def arrived(w, k):
            if mid and k == 1:
                second(w, None).wait_recv()
            else:
                across(w, k, None).wait_recv()

        def pre(k):
            at = place(0, k, 0)
            for w, target in ((0, gate_pre), (1, up_pre)):
                if k:
                    arrived(w, k)
                product = contract_last(tokens_all[:, at], whole[w][pl.ds(0, units), at])
                if k == 0:
                    target[:, :units] = product
                else:
                    target[:, :units] += product

        def start_pre():
            for copy in held:
                copy.wait()
            for w in range(3):
                mine = whole[w].at[pl.ds(0, units), place(w, 0, None)]
                pltpu.make_async_copy(mine, mine, own_sem.at[2 + w]).wait()
            complete(0)
            pre(0)

        hid_swap = remote(hid_out, hid_all.at[pl.ds(2 * rows, 2 * rows)],
                          hid_send.at[0], hid_recv.at[0], pair)

        def activate():
            gated, raw = gate_pre[:, :units], up_pre[:, :units]
            sigma = jax.nn.sigmoid(gated)
            hidden = (gated * sigma * raw).astype(BF16)
            hid_out[...] = hidden[:, sub:]
            hid_all[pl.ds(0, 2 * rows)] = hidden[:, :sub]
            gate_pre[:, :units] = gated * sigma
            up_pre[:, :units] = raw * sigma * (1.0 + gated * (1.0 - sigma))

        def add_hid(k):
            if k:
                arrived(2, k)
            else:
                complete(1)
            at = cols(other[k] * width, width)
            product = contract_last(grad_all[pl.ds(0, 2 * rows), at], down_rows(at))
            if k == 0:
                hid[:, :units] = product
            else:
                hid[:, :units] += product

        def down_rows(at):
            return whole[2][pl.ds(0, units), at]

        def d_in(k, of):
            return (d_in_m if of else d_in_e).at[k]

        def d_direct(k):
            return remote(part.at[k], d_in(k, mid), d_send.at[0], d_recv.at[k - 1], {"fs": other[k]})

        def d_done(k):
            return remote(d_in(k, role[k]), d_in(k, role[k]), d_send.at[0], d_recv.at[k - 1], {"fs": other[k]})

        def d_first(k):
            return remote(part_e.at[k], d_pass.at[k], d_send.at[0], e_recv.at[k - 2], {"fs": other[1]})

        def d_second(k):
            return remote(d_pass.at[k], d_in(k, False), e_send.at[0], d_recv.at[k - 1], {"fs": other[5 - k]})

        def products():
            complete(2)
            complete(3)
            hid_swap.wait_recv()
            for k in (2, 3, 1, 0) if mid else (3, 2, 1, 0):
                at = cols(other[k] * width, width)
                product = contract_first(hid_all[...], grad_all[:, at])
                if k == 0:
                    part_own[pl.ds(0, sub)] = product
                    continue
                part[k] = product.astype(BF16)
                (d_direct if mid or k == 1 else d_first)(k).start()

        def hand_products():
            for k in (3, 2):
                d_first(k).wait_recv()
                d_second(k).start()

        def flow(b, at):
            span = pl.ds(b * rows, rows)
            return (
                jnp.dot(gate_grad[span, :units], whole[0][pl.ds(0, units), at],
                        preferred_element_type=F32)
                + jnp.dot(up_grad[span, :units], whole[1][pl.ds(0, units), at],
                          preferred_element_type=F32)
            )

        def push(group, i, src, dst, peer):
            copy = remote(src, dst, g_send.at[group], g_recv.at[i], peer)
            copy.start()
            return copy

        def put(group, src, dst):
            pltpu.make_async_copy(src, dst, out_sem.at[group]).start()

        swaps = [
            remote(own, down_grad.at[tile(bases[of] + r * subs[of], subs[of])],
                   s_send.at[i], s_recv.at[i], pair)
            for i, (of, own) in enumerate(((True, s_own_m), (False, s_own_e)))
        ]
        sums = {}

        def rows_of(of):
            own = s_own_m if of else s_own_e
            if of == mid:
                d_done(3).wait_recv()
                own[...] = (part_own[pl.ds(0, sub)] + d_in(3, mid)[...].astype(F32)).astype(BF16)
            else:
                d_done(1).wait_recv()
                d_done(2).wait_recv()
                own[...] = (d_in(1, of)[...].astype(F32) + d_in(2, of)[...].astype(F32)).astype(BF16)
            kept = own[...].astype(F32)
            put(1, own, down_grad.at[tile(bases[of] + r * subs[of], subs[of])])
            sums[of] = lax.dot_general(
                jnp.ones((8, width), F32), kept * kept, (((1,), (1,)), ((), ())),
                precision=lax.Precision.HIGHEST, preferred_element_type=F32,
            )

        def rows_done():
            rows_of(False)
            n_own[...] = jnp.concatenate([sums[False], sums[True]], axis=1)
            for i, peer in enumerate(peers):
                remote(n_own, n_in.at[i], n_send.at[0], n_recv.at[0], peer).start()
            swaps[1].start()

        def finish_rows():
            remote(n_in, n_in, n_send.at[0], n_recv.at[0], pair).wait_recv()
            here = n_own[...]
            for i in range(n - 1):
                here = here + n_in[i]
            there = n_in[n - 1]
            for i in range(n, 2 * n - 1):
                there = there + n_in[i]
            first, later = jnp.where(r == 0, here, there), jnp.where(r == 0, there, here)
            n_sum[...] = jnp.concatenate(
                [first[:, :sub_e], later[:, :sub_e], first[:, sub_e:], later[:, sub_e:]], axis=1
            )
            put(2, n_sum, norms)
            for copy in swaps:
                copy.wait_recv()

        if mid:
            fetch(2).start()
            fetch(0).start()
            give(0, 3)
            give(1, 3)
            give(0, 1)
            fetch(1).start()
            give(1, 1)
            arrive(0, 1)
            give(0, 2)
            arrive(0, 3)
            hand(0)
            arrive(1, 3)
            hand(2)
            arrive(1, 1)
            give(1, 2)
            for k in (1, 3, 2):
                give(2, k)
            pass_on(0)
            arrive(0, 2)
            start_pre()
            hand(1)
            fetch(3).start()
            pass_on(2)
            pre(3)
            arrive(1, 2)
            pass_on(1)
            hand(3)
            arrive(2, 3)
            pre(2)
            pre(1)
            activate()
            hid_swap.start()
            pass_on(3)
            arrive(2, 1)
            add_hid(0)
            add_hid(3)
            arrive(2, 2)
            products()
            add_hid(1)
            add_hid(2)
        else:
            fetch(2).start()
            give(0, 1)
            fetch(0).start()
            give(1, 1)
            fetch(1).start()
            give(0, 3)
            give(1, 3)
            give_second(0)
            give_second(1)
            give(2, 1)
            give(2, 3)
            give_second(2)
            hand(2)
            hand(0)
            arrive(0, 1)
            pass_on(2)
            pass_on(0)
            hand(1)
            fetch(3).start()
            arrive(0, 3)
            arrive(0, 2)
            arrive(1, 1)
            arrive(1, 3)
            pass_on(1)
            start_pre()
            arrive(1, 2)
            hand(3)
            pre(1)
            pre(3)
            pass_on(3)
            arrive(2, 1)
            pre(2)
            activate()
            hid_swap.start()
            arrive(2, 2)
            add_hid(0)
            add_hid(1)
            arrive(2, 3)
            products()
            add_hid(2)
            add_hid(3)

        neighbour = {"fs": other[1]}
        cross = {}
        for b in (1, 0):
            at = pl.ds(b * rows, rows)
            up_grad[at, :units] = (hid[at, :units] * gate_pre[at, :units]).astype(BF16)
            gate_grad[at, :units] = (hid[at, :units] * up_pre[at, :units]).astype(BF16)
            f_out[b] = flow(b, cols((1 - c) * half, half)).astype(BF16)
            cross[b] = push(0, b, f_out.at[b], f_in.at[b], mate)
        mine, theirs = 2 + x, 3 - x

        def lanes(q, core=c):
            return cols(core * half + q * size, size)

        def piece(b, q):
            return flow(b, lanes(q)) + f_in[b, :, cols(q * size, size)].astype(F32)

        reduced, over = {}, []
        for b in (1, 0):
            first = flow(b, lanes(theirs))
            cross[b].wait_recv()
            x_out[b] = (first + f_in[b, :, cols(theirs * size, size)].astype(F32)).astype(BF16)
            reduced[b] = push(2, 5 + b, x_out.at[b], x_in.at[b], far)
            for q in range(2):
                if b == 1:
                    g_out[q] = piece(b, q).astype(BF16)
                    over.append(push(1, 2 + q, g_out.at[q], g_in.at[q], neighbour))
                else:
                    g_own[q] = piece(b, q)
            g_own[2 + b] = piece(b, mine)
        reduced[1].wait_recv()
        g_out[2] = (g_own[3] + x_in[1].astype(F32)).astype(BF16)
        over.append(push(1, 4, g_out.at[2], g_in.at[2], neighbour))
        if mid:
            hand_products()
        reduced[0].wait_recv()
        g_own[2] += x_in[0].astype(F32)
        sent = []
        if not mid:
            rows_of(True)
            swaps[0].start()
        for q in range(2):
            over[q].wait_recv()
            h_out[q] = (g_own[q] + g_in[q].astype(F32)).astype(BF16)
            sent.append(push(3, 7 + q, h_out.at[q], h_in.at[q], far))
            if q == 0 and mid:
                rows_of(True)
                swaps[0].start()
        if not mid:
            rows_done()
        beside = {}

        def finish(i, q):
            part_out = whole_out.at[:, lanes(q)]
            beside[i] = push(4, 10 + i, part_out, input_grad.at[:, lanes(q)], mate)
            put(0, part_out, input_grad.at[:, lanes(q)])

        over[2].wait_recv()
        whole_out[:, lanes(mine)] = (g_own[2] + g_in[2].astype(F32)).astype(BF16)
        gathered = push(5, 9, whole_out.at[:, lanes(mine)], whole_out.at[:, lanes(mine)], far)
        finish(2, mine)
        if mid:
            rows_done()
        for q in range(2):
            sent[q].wait_recv()
            whole_out[:, lanes(q)] = (h_out[q].astype(F32) + h_in[q].astype(F32)).astype(BF16)
            finish(q, q)
        finish_rows()
        gathered.wait_recv()
        finish(3, theirs)

        for w in range(3):
            for k in (1, 2, 3) if mid else (1, 3):
                weight(w, k, None).wait_send()
            (relay if mid else second)(w, None).wait_send()
            for k in (2, 3) if mid else (1, 2, 3):
                across(w, k, None).wait_send()

        def sent_all(ref, sem):
            remote(ref, ref, sem, sem, pair).wait_send()

        sent_all(grad_all, t_send.at[0])
        hid_swap.wait_send()
        sent_all(part.at[pl.ds(1, 3)], d_send.at[0])
        if mid:
            sent_all(d_pass.at[pl.ds(2, 2)], e_send.at[0])
        for i, ref in enumerate((
            f_out, g_out, x_out, h_out, whole_out.at[:, pl.ds(0, half)], whole_out.at[:, pl.ds(0, size)],
        )):
            sent_all(ref, g_send.at[i])
        sent_all(n_in, n_send.at[0])
        for copy in swaps:
            copy.wait_send()

        for i in range(4):
            beside[i].wait_recv()
        for i, (src, dst) in enumerate((
            (whole_out.at[:, pl.ds(0, half)], input_grad.at[:, pl.ds(0, half)]),
            (down_grad.at[pl.ds(0, sub_m + sub_e)], down_grad.at[pl.ds(0, sub_m + sub_e)]),
            (n_sum, norms),
        )):
            pltpu.make_async_copy(src, dst, out_sem.at[i]).wait()

    @pl.when(middle)
    def _():
        body(True)

    @pl.when(~middle)
    def _():
        body(False)


def write_kernel(flow, shard, rows, input_grad, down_grad, norms):
    input_grad[...] = flow[...]
    down_grad[...] = shard[...].astype(F32)
    norms[...] = rows[0]


def split_units(tokens, gate_weight, up_weight, down_weight, out_grad):
    rows, depth = tokens.shape
    width, both = gate_weight.shape
    sub_e = max(both * 13 // 1024, 1) * 16
    sub_m = both // 2 - sub_e
    anywhere = pl.BlockSpec(memory_space=pl.ANY)
    vmem = pl.BlockSpec(memory_space=pltpu.VMEM)
    dma = pltpu.SemaphoreType.DMA
    n, half, size = 4, depth // 2, depth // 8
    peers = 2 * n - 1
    scratch = [((2 * sub_m, depth), BF16)] * 3 + [((2 * sub_e, depth), BF16)] * 3
    scratch += [((2 * rows, depth), BF16), ((4 * rows, depth), BF16)]
    scratch += [((2 * rows, 2 * sub_m), F32)] * 3 + [((2 * rows, 2 * sub_m), BF16)] * 2
    for sub in (sub_m, sub_e):
        scratch += [((4 * rows, sub), BF16), ((2 * rows, sub), BF16)]
    scratch += [((n, sub_m, width), BF16), ((n, sub_e, width), BF16), ((sub_m, width), F32)]
    scratch += [((n, sub_m, width), BF16)] + [((n, sub_e, width), BF16)] * 2
    scratch += [((2, rows, half), BF16)] * 2 + [((4, rows, size), F32)]
    scratch += [((3, rows, size), BF16)] * 2 + [((2, rows, size), BF16)] * 4
    scratch += [((rows, depth), BF16)] + [((sub_m, width), BF16), ((sub_e, width), BF16)]
    scratch += [((8, both // 2), F32), ((peers, 8, both // 2), F32), ((8, both), F32)]
    input_grad, down_grad, norms = pl.pallas_call(
        block_kernel,
        out_shape=[
            jax.ShapeDtypeStruct((rows, depth), BF16),
            jax.ShapeDtypeStruct((both, width), BF16),
            jax.ShapeDtypeStruct((8, both), F32),
        ],
        in_specs=[anywhere] * 5,
        out_specs=[anywhere] * 3,
        scratch_shapes=[pltpu.VMEM(shape, kind) for shape, kind in scratch] + [
            dma((count,)) for count in (
                5, 9, 18, 3, 3, 3, 9, 9, 1, 12, 1, 1, 1, 3, 1, 2, 6, 14, 2, 2, 1, 1, 3,
            )
        ],
        compiler_params=pltpu.CompilerParams(collective_id=0, has_side_effects=True),
        name="block",
    )(gate_weight.T, up_weight.T, down_weight, tokens, out_grad)
    return tuple(pl.pallas_call(
        write_kernel,
        out_shape=[
            jax.ShapeDtypeStruct((rows, depth), BF16),
            jax.ShapeDtypeStruct((both, width), F32),
            jax.ShapeDtypeStruct((both,), F32),
        ],
        in_specs=[vmem] * 3,
        out_specs=[vmem] * 3,
        name="write",
    )(input_grad, down_grad, norms))


def whole_units(tokens, gate_weight, up_weight, down_weight, out_grad):
    down_full = lax.all_gather(down_weight, "fs", axis=1, tiled=True)
    gate_full = lax.all_gather(gate_weight, "fs", axis=0, tiled=True)
    up_full = lax.all_gather(up_weight, "fs", axis=0, tiled=True)
    gate_pre = jnp.dot(tokens, gate_full, preferred_element_type=F32)
    up_pre = jnp.dot(tokens, up_full, preferred_element_type=F32)
    sigma = jax.nn.sigmoid(gate_pre)
    activated = gate_pre * sigma
    hidden = (activated * up_pre).astype(BF16)
    hid_grad = contract_last(out_grad, down_full)
    up_grad = (hid_grad * activated).astype(BF16)
    gate_grad = (hid_grad * up_pre * sigma * (1.0 + gate_pre * (1.0 - sigma))).astype(BF16)
    partial_value = contract_last(gate_grad, gate_full) + contract_last(up_grad, up_full)
    input_grad = lax.psum(partial_value.astype(BF16), "tp")
    columns = lax.all_to_all(out_grad, "fs", split_axis=1, concat_axis=0, tiled=True)
    shard = contract_first(lax.all_gather(hidden, "fs", axis=0, tiled=True), columns)
    shard = lax.psum(shard.astype(BF16), "rep").astype(F32)
    norms = lax.psum(jnp.sum(shard * shard, axis=1), "fs")
    return (input_grad, shard, norms)


def solution(mesh):
    n, rep, tp = mesh.shape["fs"], mesh.shape["rep"], mesh.shape["tp"]

    def on_device(tokens, gate_weight, up_weight, down_weight, out_grad):
        width, both = gate_weight.shape
        if rep == 2 and tp == 4 and n == 4 and both % 32 == 0 and both >= 128 and width % 512 == 0 and tokens.shape[0] % 64 == 0:
            return split_units(tokens, gate_weight, up_weight, down_weight, out_grad)
        return whole_units(tokens, gate_weight, up_weight, down_weight, out_grad)

    return jax.shard_map(
        on_device,
        mesh=mesh,
        in_specs=(
            P(("rep", "fs"), None),
            P("fs", "tp"),
            P("fs", "tp"),
            P("tp", "fs"),
            P(("rep", "fs"), None),
        ),
        out_specs=(P(("rep", "fs"), None), P("tp", "fs"), P("tp")),
        check_vma=False,
    )
```

```python
import jax
import jax.numpy as jnp
from jax import lax
from jax.experimental import pallas as pl
from jax.experimental.pallas import tpu as pltpu
from jax.sharding import PartitionSpec as P

MESH = pl.DeviceIdType.MESH
BF16 = jnp.bfloat16
F32 = jnp.float32


def contract_last(left, right):
    return lax.dot_general(left, right, (((1,), (1,)), ((), ())), preferred_element_type=F32)


def contract_first(left, right):
    return lax.dot_general(left, right, (((0,), (0,)), ((), ())), preferred_element_type=F32)


def block_kernel(
    gate, up, down, tokens, grad, input_grad, down_grad, norms,
    gate_m, up_m, down_m, gate_e, up_e, down_e, tokens_all, grad_all,
    gate_pre, up_pre, hid, gate_grad, up_grad, hid_all_m, hid_out_m, hid_all_e, hid_out_e,
    part_m, part_e, part_own, d_in_m, d_in_e, d_pass,
    f_out, f_in, g_own, g_out, g_in, x_out, x_in, h_out, h_in, whole_out, s_own_m, s_own_e,
    n_own, n_in, n_sum,
    own_sem, w_send, w_recv, w_pass, b_send, b_recv, y_send, y_recv, t_send, t_recv, hid_send, hid_recv,
    d_send, d_recv, e_send, e_recv, g_send, g_recv, s_send, s_recv, n_send, n_recv, out_sem,
):
    n = 4
    f = lax.axis_index("fs")
    r = lax.axis_index("rep")
    t = lax.axis_index("tp")
    c, x = lax.rem(t, 2), t // 2
    middle = (f == 1) | (f == 2)
    mate, far, pair = {"tp": x * 2 + 1 - c}, {"tp": (1 - x) * 2 + c}, {"rep": 1 - r}
    other = (f, f + 1 - 2 * lax.rem(f, 2), lax.rem(f + 2, n), n - 1 - f)
    rows, depth = tokens.shape
    width = gate.shape[1]
    half, quarter = depth // 2, rows // 4
    size = g_out.shape[2]
    owns = (gate, up, down)
    sub_m, sub_e = hid_out_m.shape[1], hid_out_e.shape[1]
    subs = {True: sub_m, False: sub_e}
    bases = {True: 2 * sub_e, False: 0}
    wholes = {True: (gate_m, up_m, down_m), False: (gate_e, up_e, down_e)}

    def cols(start, size):
        return pl.ds(pl.multiple_of(start, size), size)

    def tile(start, size):
        return pl.ds(pl.multiple_of(start, 16), size)

    def remote(src, dst, send, recv, peer):
        return pltpu.make_async_remote_copy(
            src_ref=src, dst_ref=dst, send_sem=send, recv_sem=recv,
            device_id=peer, device_id_type=MESH,
        )

    held = [
        pltpu.make_async_copy(own, whole.at[pl.ds(0, rows)], own_sem.at[i])
        for i, (own, whole) in enumerate(((tokens, tokens_all), (grad, grad_all)))
    ]

    def own_rows(mid):
        sub = subs[mid]
        return [
            pltpu.make_async_copy(
                own.at[tile(bases[mid] + (r if b == 0 else 1 - r) * sub, sub)],
                whole.at[pl.ds(b * sub, sub), cols(f * width, width)],
                own_sem.at[2 + w],
            )
            for w, (own, whole) in enumerate(zip(owns, wholes[mid])) for b in range(2)
        ]

    for copy in held:
        copy.start()

    barrier = pltpu.get_barrier_semaphore()
    peers = [{"rep": lax.rem(r + a, 2), "fs": other[k]}
             for a in range(2) for k in range(n) if a or k]
    for peer in peers + [mate, far]:
        pl.semaphore_signal(barrier, inc=1, device_id=peer, device_id_type=MESH)
    pl.semaphore_wait(barrier, 2 * n + 1)

    cuts = (1, 1, 4)

    def slot(w, k, j):
        return w * 3 + (k - 1) * cuts[w] + j

    def place(w, k, j):
        size = width if j is None else width // cuts[w]
        return cols(other[k] * width + (0 if j is None else j * size), size)

    flows = ((tokens, tokens_all, 1), (grad, grad_all, 1), (grad, grad_all, 2), (grad, grad_all, 3))

    def span(i, q):
        return flows[i][1].at[tile(flows[i][2] * rows + q * quarter, quarter)]

    q_near, q_far = t, (1 - x) * 2 + c

    def fetch(i):
        own = grad_all.at[tile(rows + t * quarter, quarter)] if i == 3 else (
            flows[i][0].at[tile(t * quarter, quarter)])
        return remote(own, span(i, q_near), t_send.at[0], t_recv.at[i],
                      {"fs": other[1]} if i < 2 else pair)

    def spread(i, j):
        q = q_near if j < 3 else q_far
        return remote(span(i, q), span(i, q), t_send.at[0], t_recv.at[(4 if j == 1 else 8) + i],
                      far if j == 1 else mate)

    def hand(i):
        fetch(i).wait_recv()
        spread(i, 1).start()
        spread(i, 2).start()

    def pass_on(i):
        spread(i, 1).wait_recv()
        spread(i, 3).start()

    def complete(i):
        both_quarters = flows[i][1].at[pl.ds(0, 2 * quarter)]
        remote(both_quarters, both_quarters, t_send.at[0], t_recv.at[8 + i], mate).wait_recv()

    def body(mid):
        sub = subs[mid]
        units = 2 * sub
        whole = wholes[mid]
        hid_all, hid_out, part = (hid_all_m, hid_out_m, part_m) if mid else (hid_all_e, hid_out_e, part_e)
        role = (mid, not mid, not mid, mid)

        def strip(w, j):
            size = width // cuts[w]
            return pl.ds(0, width) if j is None else pl.ds(j * size, size)

        def weight(w, k, j, out=True):
            to = role[k] if out else mid
            return remote(
                owns[w].at[tile(bases[to] + r * subs[to], subs[to]), strip(w, j)],
                wholes[to][w].at[pl.ds(0, subs[to]), place(w, 0 if out else k, j)],
                w_send.at[3 * w + k - 1], w_recv.at[slot(w, k, j or 0)], {"fs": other[k]},
            )

        def second(w, j):
            return remote(
                owns[w].at[tile(bases[True] + (1 - r) * sub_m, sub_m), strip(w, j)],
                wholes[True][w].at[pl.ds(sub_m, sub_m), place(w, 1 if mid else 0, j)],
                b_send.at[w], b_recv.at[w], {"fs": other[1]},
            )

        def relay(w, j):
            held_rows = whole[w].at[pl.ds(0, sub), place(w, 1, j)]
            return remote(held_rows, held_rows, w_pass.at[w], w_recv.at[slot(w, 2, j or 0)], {"fs": other[3]})

        def across(w, k, j):
            return remote(
                whole[w].at[pl.ds(0, sub), place(w, k, j)], whole[w].at[pl.ds(sub, sub), place(w, k, j)],
                y_send.at[w], y_recv.at[3 * w + k - 1], pair,
            )

        def give(w, k):
            for j in range(cuts[w]):
                weight(w, k, j).start()

        def give_second(w):
            for j in range(cuts[w]):
                second(w, j).start()

        def arrive(w, k):
            for j in range(cuts[w]):
                weight(w, k, j, False).wait_recv()
                (relay(w, j) if mid and k == 1 else across(w, k, j)).start()

        def arrived(w, k):
            if mid and k == 1:
                second(w, None).wait_recv()
            else:
                across(w, k, None).wait_recv()

        def pre(k):
            at = place(0, k, 0)
            for w, target in ((0, gate_pre), (1, up_pre)):
                if k:
                    arrived(w, k)
                product = contract_last(tokens_all[:, at], whole[w][pl.ds(0, units), at])
                if k == 0:
                    target[:, :units] = product
                else:
                    target[:, :units] += product

        def start_pre():
            for copy in held:
                copy.wait()
            for w in range(3):
                mine = whole[w].at[pl.ds(0, units), place(w, 0, None)]
                pltpu.make_async_copy(mine, mine, own_sem.at[2 + w]).wait()
            complete(0)
            pre(0)

        hid_swap = remote(hid_out, hid_all.at[pl.ds(2 * rows, 2 * rows)],
                          hid_send.at[0], hid_recv.at[0], pair)

        def activate():
            gated, raw = gate_pre[:, :units], up_pre[:, :units]
            sigma = jax.nn.sigmoid(gated)
            hidden = (gated * sigma * raw).astype(BF16)
            hid_out[...] = hidden[:, sub:]
            hid_all[pl.ds(0, 2 * rows)] = hidden[:, :sub]
            gate_pre[:, :units] = gated * sigma
            up_pre[:, :units] = raw * sigma * (1.0 + gated * (1.0 - sigma))

        def add_hid(k):
            if k:
                arrived(2, k)
            else:
                complete(1)
            at = cols(other[k] * width, width)
            product = contract_last(grad_all[pl.ds(0, 2 * rows), at], down_rows(at))
            if k == 0:
                hid[:, :units] = product
            else:
                hid[:, :units] += product

        def down_rows(at):
            return whole[2][pl.ds(0, units), at]

        def d_in(k, of):
            return (d_in_m if of else d_in_e).at[k]

        def d_direct(k):
            return remote(part.at[k], d_in(k, mid), d_send.at[0], d_recv.at[k - 1], {"fs": other[k]})

        def d_done(k):
            return remote(d_in(k, role[k]), d_in(k, role[k]), d_send.at[0], d_recv.at[k - 1], {"fs": other[k]})

        def d_first(k):
            return remote(part_e.at[k], d_pass.at[k], d_send.at[0], e_recv.at[k - 2], {"fs": other[1]})

        def d_second(k):
            return remote(d_pass.at[k], d_in(k, False), e_send.at[0], d_recv.at[k - 1], {"fs": other[5 - k]})

        def products():
            complete(2)
            complete(3)
            hid_swap.wait_recv()
            for k in (2, 3, 1, 0) if mid else (3, 2, 1, 0):
                at = cols(other[k] * width, width)
                product = contract_first(hid_all[...], grad_all[:, at])
                if k == 0:
                    part_own[pl.ds(0, sub)] = product
                    continue
                part[k] = product.astype(BF16)
                (d_direct if mid or k == 1 else d_first)(k).start()

        def hand_products():
            for k in (3, 2):
                d_first(k).wait_recv()
                d_second(k).start()

        def flow(b, at):
            span = pl.ds(b * rows, rows)
            return (
                jnp.dot(gate_grad[span, :units], whole[0][pl.ds(0, units), at],
                        preferred_element_type=F32)
                + jnp.dot(up_grad[span, :units], whole[1][pl.ds(0, units), at],
                          preferred_element_type=F32)
            )

        def push(group, i, src, dst, peer):
            copy = remote(src, dst, g_send.at[group], g_recv.at[i], peer)
            copy.start()
            return copy

        def put(group, src, dst):
            pltpu.make_async_copy(src, dst, out_sem.at[group]).start()

        swaps = [
            remote(own, down_grad.at[tile(bases[of] + r * subs[of], subs[of])],
                   s_send.at[i], s_recv.at[i], pair)
            for i, (of, own) in enumerate(((True, s_own_m), (False, s_own_e)))
        ]
        sums = {}

        def rows_of(of):
            own = s_own_m if of else s_own_e
            if of == mid:
                d_done(3).wait_recv()
                own[...] = (part_own[pl.ds(0, sub)] + d_in(3, mid)[...].astype(F32)).astype(BF16)
            else:
                d_done(1).wait_recv()
                d_done(2).wait_recv()
                own[...] = (d_in(1, of)[...].astype(F32) + d_in(2, of)[...].astype(F32)).astype(BF16)
            kept = own[...].astype(F32)
            put(1, own, down_grad.at[tile(bases[of] + r * subs[of], subs[of])])
            sums[of] = lax.dot_general(
                jnp.ones((8, width), F32), kept * kept, (((1,), (1,)), ((), ())),
                precision=lax.Precision.HIGHEST, preferred_element_type=F32,
            )

        def rows_done():
            rows_of(False)
            n_own[...] = jnp.concatenate([sums[False], sums[True]], axis=1)
            for i, peer in enumerate(peers):
                remote(n_own, n_in.at[i], n_send.at[0], n_recv.at[0], peer).start()
            swaps[1].start()

        def finish_rows():
            remote(n_in, n_in, n_send.at[0], n_recv.at[0], pair).wait_recv()
            here = n_own[...]
            for i in range(n - 1):
                here = here + n_in[i]
            there = n_in[n - 1]
            for i in range(n, 2 * n - 1):
                there = there + n_in[i]
            first, later = jnp.where(r == 0, here, there), jnp.where(r == 0, there, here)
            n_sum[...] = jnp.concatenate(
                [first[:, :sub_e], later[:, :sub_e], first[:, sub_e:], later[:, sub_e:]], axis=1
            )
            put(2, n_sum, norms)
            for copy in swaps:
                copy.wait_recv()

        if mid:
            fetch(2).start()
            fetch(0).start()
            give(0, 3)
            give(1, 3)
            give(0, 1)
            fetch(1).start()
            give(1, 1)
            for copy in own_rows(mid):
                copy.start()
            arrive(0, 1)
            give(0, 2)
            arrive(0, 3)
            hand(0)
            arrive(1, 3)
            hand(2)
            arrive(1, 1)
            give(1, 2)
            for k in (1, 3, 2):
                give(2, k)
            pass_on(0)
            arrive(0, 2)
            start_pre()
            hand(1)
            fetch(3).start()
            pass_on(2)
            pre(3)
            arrive(1, 2)
            pass_on(1)
            hand(3)
            arrive(2, 3)
            pre(2)
            pre(1)
            activate()
            hid_swap.start()
            pass_on(3)
            arrive(2, 1)
            add_hid(0)
            add_hid(3)
            arrive(2, 2)
            products()
            add_hid(1)
            add_hid(2)
        else:
            fetch(2).start()
            give(0, 1)
            fetch(0).start()
            give(1, 1)
            fetch(1).start()
            give(0, 3)
            give(1, 3)
            give_second(0)
            give_second(1)
            give(2, 1)
            give(2, 3)
            give_second(2)
            for copy in own_rows(mid):
                copy.start()
            hand(2)
            hand(0)
            arrive(0, 1)
            pass_on(2)
            pass_on(0)
            hand(1)
            fetch(3).start()
            arrive(0, 3)
            arrive(0, 2)
            arrive(1, 1)
            arrive(1, 3)
            pass_on(1)
            start_pre()
            arrive(1, 2)
            hand(3)
            pre(1)
            pre(3)
            pass_on(3)
            arrive(2, 1)
            pre(2)
            activate()
            hid_swap.start()
            arrive(2, 2)
            add_hid(0)
            add_hid(1)
            arrive(2, 3)
            products()
            add_hid(2)
            add_hid(3)

        neighbour = {"fs": other[1]}
        cross = {}
        for b in (1, 0):
            at = pl.ds(b * rows, rows)
            up_grad[at, :units] = (hid[at, :units] * gate_pre[at, :units]).astype(BF16)
            gate_grad[at, :units] = (hid[at, :units] * up_pre[at, :units]).astype(BF16)
            f_out[b] = flow(b, cols((1 - c) * half, half)).astype(BF16)
            cross[b] = push(0, b, f_out.at[b], f_in.at[b], mate)
        mine, theirs = 2 + x, 3 - x

        def lanes(q, core=c):
            return cols(core * half + q * size, size)

        def piece(b, q):
            return flow(b, lanes(q)) + f_in[b, :, cols(q * size, size)].astype(F32)

        reduced, over = {}, []
        for b in (1, 0):
            first = flow(b, lanes(theirs))
            cross[b].wait_recv()
            x_out[b] = (first + f_in[b, :, cols(theirs * size, size)].astype(F32)).astype(BF16)
            reduced[b] = push(2, 5 + b, x_out.at[b], x_in.at[b], far)
            for q in range(2):
                if b == 1:
                    g_out[q] = piece(b, q).astype(BF16)
                    over.append(push(1, 2 + q, g_out.at[q], g_in.at[q], neighbour))
                else:
                    g_own[q] = piece(b, q)
            g_own[2 + b] = piece(b, mine)
        reduced[1].wait_recv()
        g_out[2] = (g_own[3] + x_in[1].astype(F32)).astype(BF16)
        over.append(push(1, 4, g_out.at[2], g_in.at[2], neighbour))
        if mid:
            hand_products()
        reduced[0].wait_recv()
        g_own[2] += x_in[0].astype(F32)
        sent = []
        if not mid:
            rows_of(True)
            swaps[0].start()
        for q in range(2):
            over[q].wait_recv()
            h_out[q] = (g_own[q] + g_in[q].astype(F32)).astype(BF16)
            sent.append(push(3, 7 + q, h_out.at[q], h_in.at[q], far))
            if q == 0 and mid:
                rows_of(True)
                swaps[0].start()
        if not mid:
            rows_done()
        beside = {}

        def finish(i, q):
            part_out = whole_out.at[:, lanes(q)]
            beside[i] = push(4, 10 + i, part_out, input_grad.at[:, lanes(q)], mate)
            put(0, part_out, input_grad.at[:, lanes(q)])

        over[2].wait_recv()
        whole_out[:, lanes(mine)] = (g_own[2] + g_in[2].astype(F32)).astype(BF16)
        gathered = push(5, 9, whole_out.at[:, lanes(mine)], whole_out.at[:, lanes(mine)], far)
        finish(2, mine)
        if mid:
            rows_done()
        for q in range(2):
            sent[q].wait_recv()
            whole_out[:, lanes(q)] = (h_out[q].astype(F32) + h_in[q].astype(F32)).astype(BF16)
            finish(q, q)
        finish_rows()
        gathered.wait_recv()
        finish(3, theirs)

        for w in range(3):
            for k in (1, 2, 3) if mid else (1, 3):
                weight(w, k, None).wait_send()
            (relay if mid else second)(w, None).wait_send()

        def sent_all(ref, sem):
            remote(ref, ref, sem, sem, pair).wait_send()

        for w in range(3):
            sent_all(whole[w].at[pl.ds(0, sub), pl.ds(0, (2 if mid else 3) * width)], y_send.at[w])
        sent_all(grad_all, t_send.at[0])
        hid_swap.wait_send()
        sent_all(part.at[pl.ds(1, 3)], d_send.at[0])
        if mid:
            sent_all(d_pass.at[pl.ds(2, 2)], e_send.at[0])
        for i, ref in enumerate((
            f_out, g_out, x_out, h_out, whole_out.at[:, pl.ds(0, half)], whole_out.at[:, pl.ds(0, size)],
        )):
            sent_all(ref, g_send.at[i])
        sent_all(n_in, n_send.at[0])
        for copy in swaps:
            copy.wait_send()

        for i in range(4):
            beside[i].wait_recv()
        for i, (src, dst) in enumerate((
            (whole_out.at[:, pl.ds(0, half)], input_grad.at[:, pl.ds(0, half)]),
            (down_grad.at[pl.ds(0, sub_m + sub_e)], down_grad.at[pl.ds(0, sub_m + sub_e)]),
            (n_sum, norms),
        )):
            pltpu.make_async_copy(src, dst, out_sem.at[i]).wait()

    @pl.when(middle)
    def _():
        body(True)

    @pl.when(~middle)
    def _():
        body(False)


def write_kernel(flow, shard, rows, input_grad, down_grad, norms):
    input_grad[...] = flow[...]
    down_grad[...] = shard[...].astype(F32)
    norms[...] = rows[0]


def split_units(tokens, gate_weight, up_weight, down_weight, out_grad):
    rows, depth = tokens.shape
    width, both = gate_weight.shape
    sub_e = max(both * 13 // 1024, 1) * 16
    sub_m = both // 2 - sub_e
    anywhere = pl.BlockSpec(memory_space=pl.ANY)
    vmem = pl.BlockSpec(memory_space=pltpu.VMEM)
    dma = pltpu.SemaphoreType.DMA
    n, half, size = 4, depth // 2, depth // 8
    peers = 2 * n - 1
    scratch = [((2 * sub_m, depth), BF16)] * 3 + [((2 * sub_e, depth), BF16)] * 3
    scratch += [((2 * rows, depth), BF16), ((4 * rows, depth), BF16)]
    scratch += [((2 * rows, 2 * sub_m), F32)] * 3 + [((2 * rows, 2 * sub_m), BF16)] * 2
    for sub in (sub_m, sub_e):
        scratch += [((4 * rows, sub), BF16), ((2 * rows, sub), BF16)]
    scratch += [((n, sub_m, width), BF16), ((n, sub_e, width), BF16), ((sub_m, width), F32)]
    scratch += [((n, sub_m, width), BF16)] + [((n, sub_e, width), BF16)] * 2
    scratch += [((2, rows, half), BF16)] * 2 + [((4, rows, size), F32)]
    scratch += [((3, rows, size), BF16)] * 2 + [((2, rows, size), BF16)] * 4
    scratch += [((rows, depth), BF16)] + [((sub_m, width), BF16), ((sub_e, width), BF16)]
    scratch += [((8, both // 2), F32), ((peers, 8, both // 2), F32), ((8, both), F32)]
    input_grad, down_grad, norms = pl.pallas_call(
        block_kernel,
        out_shape=[
            jax.ShapeDtypeStruct((rows, depth), BF16),
            jax.ShapeDtypeStruct((both, width), BF16),
            jax.ShapeDtypeStruct((8, both), F32),
        ],
        in_specs=[anywhere] * 5,
        out_specs=[anywhere] * 3,
        scratch_shapes=[pltpu.VMEM(shape, kind) for shape, kind in scratch] + [
            dma((count,)) for count in (
                5, 9, 18, 3, 3, 3, 3, 9, 1, 12, 1, 1, 1, 3, 1, 2, 6, 14, 2, 2, 1, 1, 3,
            )
        ],
        compiler_params=pltpu.CompilerParams(collective_id=0, has_side_effects=True),
        name="block",
    )(gate_weight.T, up_weight.T, down_weight, tokens, out_grad)
    return tuple(pl.pallas_call(
        write_kernel,
        out_shape=[
            jax.ShapeDtypeStruct((rows, depth), BF16),
            jax.ShapeDtypeStruct((both, width), F32),
            jax.ShapeDtypeStruct((both,), F32),
        ],
        in_specs=[vmem] * 3,
        out_specs=[vmem] * 3,
        name="write",
    )(input_grad, down_grad, norms))


def whole_units(tokens, gate_weight, up_weight, down_weight, out_grad):
    down_full = lax.all_gather(down_weight, "fs", axis=1, tiled=True)
    gate_full = lax.all_gather(gate_weight, "fs", axis=0, tiled=True)
    up_full = lax.all_gather(up_weight, "fs", axis=0, tiled=True)
    gate_pre = jnp.dot(tokens, gate_full, preferred_element_type=F32)
    up_pre = jnp.dot(tokens, up_full, preferred_element_type=F32)
    sigma = jax.nn.sigmoid(gate_pre)
    activated = gate_pre * sigma
    hidden = (activated * up_pre).astype(BF16)
    hid_grad = contract_last(out_grad, down_full)
    up_grad = (hid_grad * activated).astype(BF16)
    gate_grad = (hid_grad * up_pre * sigma * (1.0 + gate_pre * (1.0 - sigma))).astype(BF16)
    partial_value = contract_last(gate_grad, gate_full) + contract_last(up_grad, up_full)
    input_grad = lax.psum(partial_value.astype(BF16), "tp")
    columns = lax.all_to_all(out_grad, "fs", split_axis=1, concat_axis=0, tiled=True)
    shard = contract_first(lax.all_gather(hidden, "fs", axis=0, tiled=True), columns)
    shard = lax.psum(shard.astype(BF16), "rep").astype(F32)
    norms = lax.psum(jnp.sum(shard * shard, axis=1), "fs")
    return (input_grad, shard, norms)


def solution(mesh):
    n, rep, tp = mesh.shape["fs"], mesh.shape["rep"], mesh.shape["tp"]

    def on_device(tokens, gate_weight, up_weight, down_weight, out_grad):
        width, both = gate_weight.shape
        if rep == 2 and tp == 4 and n == 4 and both % 32 == 0 and both >= 128 and width % 512 == 0 and tokens.shape[0] % 64 == 0:
            return split_units(tokens, gate_weight, up_weight, down_weight, out_grad)
        return whole_units(tokens, gate_weight, up_weight, down_weight, out_grad)

    return jax.shard_map(
        on_device,
        mesh=mesh,
        in_specs=(
            P(("rep", "fs"), None),
            P("fs", "tp"),
            P("fs", "tp"),
            P("tp", "fs"),
            P(("rep", "fs"), None),
        ),
        out_specs=(P(("rep", "fs"), None), P("tp", "fs"), P("tp")),
        check_vma=False,
    )
```
